256 devices in a mesh: tp: 256 (over z, y, x, core).
Axes of the slice: x: 4, y: 4, z: 8, core: 2. Of those that a mesh axis runs over, the one named last changes fastest.
Arguments:
- tokens: bfloat16 [32, 4096], replicated, may hold values from -18 to 18
- norm_gain: float32 [2, 4096], replicated, may hold values from 0.1 to 1.9
- w_gate: bfloat16 [2, 4096, 8192], P(None, None, 'tp'), may hold values from -0.09375 to 0.09375
- w_value: bfloat16 [2, 4096, 8192], P(None, None, 'tp'), may hold values from -0.09375 to 0.09375
- w_write: bfloat16 [2, 4096, 1024], P(None, None, 'tp'), may hold values from -0.09375 to 0.09375
- w_read: bfloat16 [2, 4096, 1024], P(None, None, 'tp'), may hold values from -0.09375 to 0.09375
- w_step: bfloat16 [2, 4096, 128], replicated, may hold values from -0.09375 to 0.09375
- step_bias: float32 [2, 128], replicated, may hold values from -2 to 1
- decay_rate: float32 [2, 128], replicated, may hold values from 0.05 to 3
- skip_gain: float32 [2, 128], replicated, may hold values from 1 to 4
- conv_value_weight: float32 [2, 3, 8192], P(None, None, 'tp'), may hold values from -2.5 to 2.5
- conv_key_weight: float32 [2, 3, 2, 1024], P(None, None, None, 'tp'), may hold values from -2.5 to 2.5
- group_gain: float32 [2, 8192], P(None, 'tp'), may hold values from 0.1 to 1.9
- w_out: bfloat16 [2, 8192, 4096], P(None, 'tp'), may hold values from -0.0625 to 0.0625
- ssm_state: float32 [2, 32, 8192, 128], P(None, None, 'tp'), may hold values from -3 to 3
- conv_value: float32 [2, 32, 2, 8192], P(None, None, None, 'tp'), may hold values from -5 to 5
- conv_key: float32 [2, 32, 2, 2, 1024], P(None, None, None, None, 'tp'), may hold values from -5 to 5
Outputs:
- tokens_out: bfloat16 [32, 4096], replicated
- ssm_state_out: float32 [2, 32, 8192, 128], P(None, None, 'tp')
- conv_value_out: float32 [2, 32, 2, 8192], P(None, None, None, 'tp')
- conv_key_out: float32 [2, 32, 2, 2, 1024], P(None, None, None, None, 'tp')
The draws below stay inside these ranges and needn't reach their ends.
All inputs are finite; a program needn't handle non-finite values.
Results may differ from the reference program's by a relative error of at most 0.011.
Values may be sent and summed in bfloat16 or wider, within the bound.
No kernel may reach another device: no remote copies, remote signals or barrier semaphores. Data moves between devices by JAX's collectives and lax.ppermute only.
A program may use at most 64 MiB of HBM per device.

```python
import math
import jax
import jax.numpy as jnp
from jax import lax

D = 4096
SSDW = 8192
HEAD_DIM = 64
GROUPS = 8
STATE = 128
CONV = 3
LAYERS = 2
BATCH = 32
HEADS = 128
HPG = 16
GW = 1024


def draw_tokens(key, part):
    key_scale, key_value = jax.random.split(key)
    column_scale = jnp.exp(jax.random.uniform(key_scale, (1, D), jnp.float32, math.log(0.3), math.log(3.0)))
    values = jnp.clip(jax.random.normal(key_value, (BATCH, D), jnp.float32), -6.0, 6.0)
    return (values * column_scale).astype(jnp.bfloat16)


def levels(stream_key, dims, cuts, smallest, high):
    gain, own = 1.0, jax.random.fold_in(stream_key, 6)
    for axis_at, shards_of in cuts:
        heights = jnp.exp(jax.random.uniform(jax.random.fold_in(own, axis_at), (shards_of,), jnp.float32, smallest / len(cuts), high / len(cuts)))
        gain = gain * jnp.repeat(heights, dims[axis_at] // shards_of).reshape([-1 if axis == axis_at else 1 for axis in range(len(dims))])
    return gain


def noise(own_key, shape, deviation, most, pieces=(), kind=jnp.bfloat16):
    result = deviation * jax.random.normal(own_key, shape, jnp.float32)
    if pieces:
        result = result * levels(own_key, shape, pieces, -0.22, 0.18)
    return jnp.clip(result, -most, most).astype(kind)


def setup_inputs(seed: int = 0) -> dict:
    streams_of = jax.random.split(jax.random.key(seed), 18)
    tokens = draw_tokens(jax.random.fold_in(streams_of[17], 71), 0)
    norm_gain = jnp.clip(1.0 + 0.18 * jax.random.normal(streams_of[1], (LAYERS, D), jnp.float32), 0.1, 1.9)
    w_gate = noise(streams_of[2], (LAYERS, D, SSDW), D ** -0.5, 0.09375, ((2, 256),))
    w_value = noise(streams_of[3], (LAYERS, D, SSDW), D ** -0.5, 0.09375, ((2, 256),))
    w_write = noise(streams_of[4], (LAYERS, D, GROUPS * STATE), D ** -0.5, 0.09375, ((2, 256),))
    w_read = noise(streams_of[5], (LAYERS, D, GROUPS * STATE), D ** -0.5, 0.09375, ((2, 256),))
    w_step = noise(streams_of[6], (LAYERS, D, HEADS), D ** -0.5, 0.09375)
    step_bias = jnp.clip(jax.random.uniform(streams_of[7], (LAYERS, HEADS), jnp.float32, -2.0, 1.0), -2.0, 1.0)
    decay_rate = jnp.clip(jnp.exp(jax.random.uniform(streams_of[8], (LAYERS, HEADS), jnp.float32, math.log(0.05), math.log(3.0))), 0.05, 3.0)
    skip_gain = jnp.clip(jnp.exp(jax.random.uniform(streams_of[9], (LAYERS, HEADS), jnp.float32, math.log(1.0), math.log(4.0))), 1.0, 4.0)
    conv_value_weight = noise(streams_of[10], (LAYERS, CONV, SSDW), 0.577, 2.5, ((2, 256),), jnp.float32)
    conv_key_weight = noise(streams_of[11], (LAYERS, CONV, 2, GROUPS * STATE), 0.577, 2.5, ((3, 256),), jnp.float32)
    group_gain = jnp.clip(1.0 + 0.18 * jax.random.normal(streams_of[12], (LAYERS, SSDW), jnp.float32), 0.1, 1.9)
    w_out = noise(streams_of[13], (LAYERS, SSDW, D), SSDW ** -0.5, 0.0625, ((1, 256),))
    ssm_state = noise(streams_of[14], (LAYERS, BATCH, SSDW, STATE), 0.5, 3.0, ((2, 256),), jnp.float32)
    conv_value = noise(streams_of[15], (LAYERS, BATCH, CONV - 1, SSDW), 1.0, 5.0, ((3, 256),), jnp.float32)
    conv_key = noise(streams_of[16], (LAYERS, BATCH, CONV - 1, 2, GROUPS * STATE), 1.0, 5.0, ((4, 256),), jnp.float32)
    return {"tokens": tokens, "norm_gain": norm_gain, "w_gate": w_gate, "w_value": w_value, "w_write": w_write, "w_read": w_read, "w_step": w_step, "step_bias": step_bias, "decay_rate": decay_rate, "skip_gain": skip_gain, "conv_value_weight": conv_value_weight, "conv_key_weight": conv_key_weight, "group_gain": group_gain, "w_out": w_out, "ssm_state": ssm_state, "conv_value": conv_value, "conv_key": conv_key}


EPS = 1e-06

def reference(tokens, norm_gain, w_gate, w_value, w_write, w_read, w_step, step_bias, decay_rate, skip_gain, conv_value_weight, conv_key_weight, group_gain, w_out, ssm_state, conv_value, conv_key):
    hidden = tokens
    ssm_list = []
    value_list = []
    key_list = []
    for layer in range(LAYERS):
        resid = hidden.astype(jnp.float32)
        inv_scale = lax.rsqrt(lax.optimization_barrier(jnp.sum(resid * resid, axis=1)) / D + EPS)[:, None]
        scaled = (resid * norm_gain[layer]).astype(jnp.bfloat16)

        def project(weight):
            return jnp.dot(scaled, weight[layer], preferred_element_type=jnp.float32) * inv_scale
        gate_in = project(w_gate)
        value_in = project(w_value)
        write_in = project(w_write)
        read_in = project(w_read)
        step_in = project(w_step)
        value_window = jnp.concatenate([conv_value[layer], value_in[:, None, :]], axis=1)
        value_list.append(value_window[:, 1:])
        values = jax.nn.silu(lax.optimization_barrier(jnp.sum(value_window * conv_value_weight[layer][None], axis=1)))
        values = values.reshape(BATCH, GROUPS, HPG, HEAD_DIM)
        fresh = jnp.stack([write_in, read_in], axis=1)[:, None]
        key_window = jnp.concatenate([conv_key[layer], fresh], axis=1)
        key_list.append(key_window[:, 1:])
        mixed_keys = jax.nn.silu(lax.optimization_barrier(jnp.sum(key_window * conv_key_weight[layer][None], axis=1)))
        writes = jnp.transpose(mixed_keys[:, 0].reshape(BATCH, STATE, GROUPS), (0, 2, 1))
        reads = jnp.transpose(mixed_keys[:, 1].reshape(BATCH, STATE, GROUPS), (0, 2, 1))
        delta = jax.nn.softplus(step_in + step_bias[layer][None])
        decay = jnp.exp(-delta * decay_rate[layer][None])
        delta = delta.reshape(BATCH, GROUPS, HPG)
        decay = decay.reshape(BATCH, GROUPS, HPG)
        state = ssm_state[layer].reshape(BATCH, GROUPS, HPG, HEAD_DIM, STATE)
        state = decay[..., None, None] * state + (delta[..., None] * values)[..., None] * writes[:, :, None, None, :]
        ssm_list.append(state.reshape(BATCH, SSDW, STATE))
        read_out = jnp.einsum('bghpn,bgn->bghp', state, reads, precision=lax.Precision.HIGHEST)
        read_out = read_out + skip_gain[layer].reshape(GROUPS, HPG)[None, :, :, None] * values
        gated = read_out.reshape(BATCH, GROUPS, GW) * jax.nn.silu(gate_in.reshape(BATCH, GROUPS, GW))
        group_scale = lax.rsqrt(lax.optimization_barrier(jnp.mean(gated * gated, axis=2, keepdims=True)) + EPS)
        normed = (gated * group_scale * group_gain[layer].reshape(GROUPS, GW)[None]).astype(jnp.bfloat16)
        update = jnp.dot(normed.reshape(BATCH, SSDW), w_out[layer], preferred_element_type=jnp.float32)
        hidden = (resid + update).astype(jnp.bfloat16)
    return (hidden, jnp.stack(ssm_list), jnp.stack(value_list), jnp.stack(key_list))
```

```python
import functools

import jax
import jax.numpy as jnp
from jax import lax
from jax.experimental import pallas as pl
from jax.experimental.pallas import tpu as pltpu
from jax.sharding import Mesh
from jax.sharding import PartitionSpec as P

D = 4096
B = 32
CH = 32
N = 128
GW = 1024
EPS = 1e-06
TP = ("z", "y", "x", "c")
PLANE = ("y", "x", "c")
F32 = jnp.float32
BF16 = jnp.bfloat16


def vmem():
    return pl.BlockSpec(memory_space=pltpu.VMEM)


def anywhere():
    return pl.BlockSpec(memory_space=pl.ANY)


def shaped(shape, dtype):
    return jax.ShapeDtypeStruct(shape, dtype)


def silu(v):
    return v / (1.0 + jnp.exp(-v))


def as_col(row):
    n = row.shape[1]
    at = lax.broadcasted_iota(jnp.int32, (n, n), 0)
    of = lax.broadcasted_iota(jnp.int32, (n, n), 1)
    return jnp.sum(jnp.where(at == of, row, 0.0), axis=1, keepdims=True)


def as_row(col):
    n = col.shape[0]
    at = lax.broadcasted_iota(jnp.int32, (n, n), 0)
    of = lax.broadcasted_iota(jnp.int32, (n, n), 1)
    return jnp.sum(jnp.where(at == of, col, 0.0), axis=0, keepdims=True)


def dot_nt(a, b):
    return lax.dot_general(a, b, (((1,), (1,)), ((), ())), preferred_element_type=F32)


def keys_kernel(layer, spot, hid, gain, w_write, w_read, conv, taps, *rest):
    if layer:
        before, msg, conv_out, scaled, inv_out = rest
    else:
        msg, conv_out, scaled, inv_out = rest
    squares = jnp.zeros((B, 128), F32)
    for j in range(D // 128):
        cols = slice(128 * j, 128 * j + 128)
        part = (hid[j] if layer else hid[:, cols]).astype(F32)
        squares += part * part
        scaled[:, cols] = (part * gain[layer : layer + 1, cols]).astype(BF16)
    inv = lax.rsqrt(jnp.sum(squares, axis=1, keepdims=True) / D + EPS)
    inv_out[...] = jnp.broadcast_to(inv, (B, 128))
    inv_row = as_row(inv)
    mixed = []
    for kind, weight in ((0, w_write), (1, w_read)):
        fresh = dot_nt(weight[layer], scaled[...]) * inv_row
        old, newer = conv[layer, 0, kind], conv[layer, 1, kind]
        tap = [as_col(taps[layer, k, kind : kind + 1, :]) for k in range(3)]
        mixed.append(silu(old * tap[0] + newer * tap[1] + fresh * tap[2]))
        if layer:
            conv_out[0, 0, kind] = before[0, kind]
            conv_out[0, 1, kind] = before[1, kind]
            conv_out[1, 0, kind] = newer
            conv_out[1, 1, kind] = fresh
        else:
            conv_out[0, kind] = newer
            conv_out[1, kind] = fresh
    lines = jnp.concatenate([mixed[0], mixed[1], jnp.zeros((4, 128 - 2 * B), F32)], axis=1)
    core = spot[2]
    for plane in range(8):
        line = lines[plane % 4 : plane % 4 + 1]
        line = jnp.where(core == plane // 4, line, 0.0)
        block = jnp.broadcast_to(line, (16, 128))
        msg[0, plane] = block
        msg[1, plane] = block


def make_keys(layer, spot, hid, gain, w_write, w_read, conv, taps, before):
    args = [spot, hid, gain, w_write, w_read, conv, taps]
    conv_shape = (2, 2, 4, B)
    if layer:
        args.append(before)
        conv_shape = (2, *conv_shape)
    return pl.pallas_call(
        functools.partial(keys_kernel, layer),
        in_specs=[pl.BlockSpec(memory_space=pltpu.SMEM)] + [vmem()] * (len(args) - 1),
        out_specs=[vmem()] * 4,
        out_shape=[
            shaped((2, 8, 16, 128), F32),
            shaped(conv_shape, F32),
            shaped((B, D), BF16),
            shaped((B, 128), F32),
        ],
        name=f"keys{layer}",
    )(*args)


def values_kernel(layer, spot, scaled, inv, w_gate, w_value, w_step, bias, rate, skip, conv, taps, *rest):
    if layer:
        before, packed, conv_out = rest
    else:
        packed, conv_out = rest
    hidden = scaled[...]
    inv_col = inv[:, :CH]
    gate = dot_nt(hidden, w_gate[layer]) * inv_col
    fresh = dot_nt(hidden, w_value[layer]) * inv_col
    step = jnp.dot(hidden, w_step[layer], preferred_element_type=F32) * inv[...]
    old, newer = conv[layer, :, 0, :], conv[layer, :, 1, :]
    tap = [taps[k, layer : layer + 1, :] for k in range(3)]
    values = silu(old * tap[0] + newer * tap[1] + fresh * tap[2])
    if layer:
        conv_out[0] = before[...]
        conv_out[1, :, 0, :] = newer
        conv_out[1, :, 1, :] = fresh
    else:
        conv_out[:, 0, :] = newer
        conv_out[:, 1, :] = fresh
    head = spot[1]
    mine = lax.broadcasted_iota(jnp.int32, (1, 128), 1) == head

    def of_head(table):
        return jnp.sum(jnp.where(mine, table, 0.0), axis=1, keepdims=True)

    raw = of_head(step + bias[layer : layer + 1, :])
    delta = jnp.maximum(raw, 0.0) + jnp.log1p(jnp.exp(-jnp.abs(raw)))
    decay = jnp.exp(-delta * of_head(rate[layer : layer + 1, :]))
    packed[0] = (delta * values).T
    packed[1] = of_head(skip[layer : layer + 1, :]) * values
    packed[2] = silu(gate)
    packed[3] = jnp.broadcast_to(decay, (B, CH))


def make_values(layer, spot, scaled, inv, w_gate, w_value, w_step, bias, rate, skip, conv, taps, before):
    args = [spot, scaled, inv, w_gate, w_value, w_step, bias, rate, skip, conv, taps]
    specs = [pl.BlockSpec(memory_space=pltpu.SMEM), vmem(), vmem()]
    specs += [vmem()] * 8
    conv_shape = (B, 2, CH)
    if layer:
        args.append(before)
        specs.append(vmem())
        conv_shape = (2, *conv_shape)
    return pl.pallas_call(
        functools.partial(values_kernel, layer),
        in_specs=specs,
        out_specs=[vmem()] * 2,
        out_shape=[shaped((4, B, CH), F32), shaped(conv_shape, F32)],
        name=f"values{layer}",
    )(*args)


def mix_kernel(layer, keys, packed, state, gain, w_out, *rest):
    states_out, sent, fresh, sem = rest[-4:]
    both = (keys[0] + keys[1]).T
    writes, reads = both[:B], both[B : 2 * B]
    push = packed[0]
    decay = packed[3]
    lane = lax.broadcasted_iota(jnp.int32, (CH, B), 1)
    found = jnp.zeros((CH, B), F32)
    for b in range(B):
        new = decay[b : b + 1, :1] * state[layer, b] + push[:, b : b + 1] * writes[b : b + 1]
        fresh[b] = new
        total = jnp.sum(new * reads[b : b + 1], axis=1, keepdims=True)
        found = jnp.where(lane == b, total, found)
    write_back = pltpu.make_async_copy(fresh, states_out.at[layer], sem)
    write_back.start()
    gated = (found.T + packed[1]) * packed[2]
    total = as_row(jnp.sum(gated * gated, axis=1, keepdims=True))
    high = total.astype(BF16).astype(F32)
    low = total - high
    row = lax.broadcasted_iota(jnp.int32, (8, B), 0)
    tail = jnp.where(row == 0, high, jnp.where(row == 1, low, 0.0))
    tail = jnp.concatenate([tail, jnp.zeros((8, 128 - B), F32)], axis=1).astype(BF16)
    out = jnp.dot((gated * gain[layer : layer + 1, :]).astype(BF16), w_out[layer], preferred_element_type=F32)
    for j in range(D // 128):
        sent[j, :B] = out[:, 128 * j : 128 * j + 128].astype(BF16)
        sent[j, B:] = tail
    write_back.wait()


def make_mix(layer, keys, packed, state, gain, w_out, states_out):
    args = [keys, packed, state, gain, w_out]
    specs = [vmem()] * 5
    aliases = {}
    if layer:
        args.append(states_out)
        specs.append(anywhere())
        aliases = {5: 0}
    return pl.pallas_call(
        functools.partial(mix_kernel, layer),
        in_specs=specs,
        out_specs=[anywhere(), vmem()],
        out_shape=[shaped(state.shape, F32), shaped((32, 40, 128), BF16)],
        scratch_shapes=[pltpu.VMEM((B, CH, N), F32), pltpu.SemaphoreType.DMA],
        input_output_aliases=aliases,
        name=f"mix{layer}",
    )(*args)


def scale_kernel(got, sent):
    total = got[0].astype(F32)
    for j in range(1, 32):
        total += got[j].astype(F32)
    squares = total[B : B + 1, :B] + total[B + 1 : B + 2, :B]
    factor = as_col(lax.rsqrt(squares / GW + EPS))
    chunk = (total[:B] * factor).astype(BF16)
    for plane in range(8):
        sent[plane] = chunk


def make_scale(got):
    return pl.pallas_call(
        scale_kernel,
        in_specs=[vmem()],
        out_specs=vmem(),
        out_shape=shaped((8, B, 128), BF16),
        name="scale",
    )(got)


def add_kernel(layer, spot, got, hid, sent):
    total = got[0].astype(F32)
    for plane in range(1, 8):
        total += got[plane].astype(F32)
    at = spot[0]
    if layer:
        own = hid[at]
    else:
        own = hid[:, pl.ds(pl.multiple_of(128 * at, 128), 128)]
    chunk = (own.astype(F32) + total).astype(BF16)
    for j in range(32):
        sent[j] = chunk


def make_add(layer, spot, got, hid):
    return pl.pallas_call(
        functools.partial(add_kernel, layer),
        in_specs=[pl.BlockSpec(memory_space=pltpu.SMEM), vmem(), vmem()],
        out_specs=vmem(),
        out_shape=shaped((32, B, 128), BF16),
        name=f"add{layer}",
    )(spot, got, hid)


def exchange(value, axes):
    return lax.all_to_all(value, axes, split_axis=0, concat_axis=0, tiled=True)


def per_device(
    tokens,
    norm_gain,
    w_gate,
    w_value,
    w_write,
    w_read,
    w_step,
    step_bias,
    decay_rate,
    skip_gain,
    conv_value_weight,
    conv_key_weight,
    group_gain,
    w_out,
    ssm_state,
    conv_value,
    conv_key,
):
    core = lax.axis_index("c")
    place = lax.axis_index(PLANE)
    head = lax.axis_index(("z", "y", "x"))
    spot = jnp.stack([place, head, core]).astype(jnp.int32)
    w_gate, w_value, w_write, w_read = (jnp.swapaxes(w, 1, 2) for w in (w_gate, w_value, w_write, w_read))
    conv_key = jnp.transpose(conv_key, (0, 2, 3, 4, 1))
    value_taps = jnp.swapaxes(conv_value_weight, 0, 1)
    hid = tokens
    states = key_out = value_out = None
    for layer in range(2):
        msg, key_out, scaled, inv = make_keys(
            layer, spot, hid, norm_gain, w_write, w_read, conv_key, conv_key_weight, key_out
        )
        keys = exchange(msg.reshape(256, 128), ("c", "z", "y", "x")).reshape(2, 128, 128)
        packed, value_out = make_values(
            layer, spot, scaled, inv, w_gate, w_value, w_step, step_bias, decay_rate, skip_gain,
            conv_value, value_taps, value_out,
        )
        states, sent = make_mix(layer, keys, packed, ssm_state, group_gain, w_out, states)
        sent = make_scale(exchange(sent, PLANE))
        sent = make_add(layer, spot, exchange(sent, ("z",)), hid)
        hid = exchange(sent, PLANE)
    tokens_out = jnp.transpose(hid, (1, 0, 2)).reshape(B, D)
    return (tokens_out, states, value_out, jnp.transpose(key_out, (0, 4, 1, 2, 3)))


def solution(mesh):
    torus = Mesh(mesh.devices.reshape(8, 4, 4, 2), TP)
    in_specs = (
        P(),
        P(),
        P(None, None, TP),
        P(None, None, TP),
        P(None, None, TP),
        P(None, None, TP),
        P(),
        P(),
        P(),
        P(),
        P(None, None, TP),
        P(None, None, None, TP),
        P(None, TP),
        P(None, TP, None),
        P(None, None, TP, None),
        P(None, None, None, TP),
        P(None, None, None, None, TP),
    )
    out_specs = (
        P(),
        P(None, None, TP, None),
        P(None, None, None, TP),
        P(None, None, None, None, TP),
    )
    return jax.shard_map(
        per_device, mesh=torus, in_specs=in_specs, out_specs=out_specs, check_vma=False
    )
```

```python
import functools

import jax
import jax.numpy as jnp
from jax import lax
from jax.experimental import pallas as pl
from jax.experimental.pallas import tpu as pltpu
from jax.sharding import Mesh
from jax.sharding import PartitionSpec as P

D = 4096
B = 32
CH = 32
N = 128
GW = 1024
EPS = 1e-06
TP = ("z", "y", "x", "c")
PLANE = ("y", "x", "c")
F32 = jnp.float32
BF16 = jnp.bfloat16


LIMIT = pltpu.CompilerParams(vmem_limit_bytes=8 * 1024 * 1024)
LINES = (2, 8, 16, 128)


def vmem():
    return pl.BlockSpec(memory_space=pltpu.VMEM)


def anywhere():
    return pl.BlockSpec(memory_space=pl.ANY)


def shaped(shape, dtype):
    return jax.ShapeDtypeStruct(shape, dtype)


def start_all(pairs, sems):
    copies = [pltpu.make_async_copy(src, dst, sems.at[at]) for at, (src, dst) in enumerate(pairs)]
    for copy in copies:
        copy.start()
    return copies


def call(body, name, near, far, outs, scratch=(), aliases=None):
    near = [pltpu.with_memory_space_constraint(v, pltpu.VMEM) for v in near]
    far = [pltpu.with_memory_space_constraint(v, pltpu.HBM) for v in far]
    far_out = (pltpu.HBM((1,), F32).memory_space,)
    specs = [anywhere() if getattr(o, "memory_space", None) in far_out else vmem() for o in outs]
    return pl.pallas_call(
        body,
        in_specs=[vmem()] * len(near) + [anywhere()] * len(far),
        out_specs=specs,
        out_shape=list(outs),
        scratch_shapes=list(scratch),
        input_output_aliases=aliases or {},
        compiler_params=LIMIT,
        name=name,
    )(*near, *far)


def silu(v):
    return v / (1.0 + jnp.exp(-v))


def as_col(row):
    n = row.shape[1]
    at = lax.broadcasted_iota(jnp.int32, (n, n), 0)
    of = lax.broadcasted_iota(jnp.int32, (n, n), 1)
    return jnp.sum(jnp.where(at == of, row, 0.0), axis=1, keepdims=True)


def as_row(col):
    n = col.shape[0]
    at = lax.broadcasted_iota(jnp.int32, (n, n), 0)
    of = lax.broadcasted_iota(jnp.int32, (n, n), 1)
    return jnp.sum(jnp.where(at == of, col, 0.0), axis=0, keepdims=True)


def dot_nt(a, b):
    return lax.dot_general(a, b, (((1,), (1,)), ((), ())), preferred_element_type=F32)


def write_keys(part_of, near, msg, conv_out, scaled, inv_out):
    gain, w_write, w_read, conv, taps = near
    squares = jnp.zeros((B, 128), F32)
    for j in range(D // 128):
        cols = slice(128 * j, 128 * j + 128)
        part = part_of(j).astype(F32)
        squares += part * part
        scaled[:, cols] = (part * gain[:, cols]).astype(BF16)
    inv = lax.rsqrt(jnp.sum(squares, axis=1, keepdims=True) / D + EPS)
    inv_out[...] = jnp.broadcast_to(inv, (B, 128))
    inv_row = as_row(inv)
    mixed = []
    for kind, weight in ((0, w_write), (1, w_read)):
        fresh = dot_nt(weight[...], scaled[...]) * inv_row
        old, newer = conv[0, kind], conv[1, kind]
        tap = [as_col(taps[k, kind : kind + 1, :]) for k in range(3)]
        mixed.append(silu(old * tap[0] + newer * tap[1] + fresh * tap[2]))
        conv_out[0, kind] = newer
        conv_out[1, kind] = fresh
    lines = jnp.concatenate([mixed[0], mixed[1], jnp.zeros((4, 128 - 2 * B), F32)], axis=1)
    core = lax.axis_index("c")
    for plane in range(8):
        line = lines[plane % 4 : plane % 4 + 1]
        line = jnp.where(core == plane // 4, line, 0.0)
        block = jnp.broadcast_to(line, (16, 128))
        msg[0, plane] = block
        msg[1, plane] = block


KEY_PARAMS = (((1, D), F32), ((4, D), BF16), ((4, D), BF16), ((2, 2, 4, B), F32), ((3, 2, 4), F32))


def key_pairs(layer, far, near):
    gain, w_write, w_read, conv, taps = far
    source = (gain.at[layer : layer + 1], w_write.at[layer], w_read.at[layer], conv.at[layer], taps.at[layer])
    return list(zip(source, near))


def first_keys_kernel(tokens, *refs):
    far, (msg, conv_out, scaled, inv_out, hid), near, sems = refs[:5], refs[5:10], refs[10:15], refs[15]
    for copy in start_all([(tokens, hid)] + key_pairs(0, far, near), sems):
        copy.wait()
    write_keys(lambda j: hid[:, 128 * j : 128 * j + 128], near, msg, conv_out, scaled, inv_out)


def first_keys(tokens, params):
    return call(
        first_keys_kernel,
        "keys0",
        [],
        [tokens, *params],
        [
            shaped(LINES, F32),
            pltpu.VMEM((2, 2, 4, B), F32),
            pltpu.VMEM((B, D), BF16),
            pltpu.VMEM((B, 128), F32),
            pltpu.VMEM((B, D), BF16),
        ],
        [pltpu.VMEM(*p) for p in KEY_PARAMS] + [pltpu.SemaphoreType.DMA((6,))],
    )


def next_keys_kernel(hid, *refs):
    near, before, (msg, conv_out, scaled, inv_out) = refs[:5], refs[5], refs[6:]
    conv_out[0] = before[...]
    write_keys(lambda j: hid[j], near, msg, conv_out.at[1], scaled, inv_out)


def next_keys(hid, near, before):
    return call(
        next_keys_kernel,
        "keys1",
        [hid, *near, before],
        [],
        [
            shaped(LINES, F32),
            shaped((2, 2, 2, 4, B), F32),
            pltpu.VMEM((B, D), BF16),
            pltpu.VMEM((B, 128), F32),
        ],
    )


VALUE_PARAMS = (
    ((CH, D), BF16),
    ((CH, D), BF16),
    ((D, 128), BF16),
    ((2, 128), F32),
    ((2, 128), F32),
    ((2, 128), F32),
    ((B, 2, CH), F32),
    ((3, 2, CH), F32),
)
MIX_PARAMS = (((B, CH, N), F32), ((CH, D), BF16), ((2, CH), F32))


def values_kernel(layer, scaled, inv, *refs):
    refs = list(refs)

    def take(n):
        got = refs[:n]
        del refs[:n]
        return got

    before = take(layer)
    far, mix_far, key_far = take(8), take(3), take(0 if layer else 5)
    (packed, conv_out), mix_near, key_near = take(2), take(3), take(0 if layer else 5)
    near, (sems, late_sems) = take(8), take(2)
    gate_far, value_far, step_far, bias, rate, skip, conv_far, taps_far = far
    state, w_out, gain = mix_far
    source = (gate_far.at[layer], value_far.at[layer], step_far.at[layer], bias, rate, skip, conv_far.at[layer], taps_far)
    copies = start_all(list(zip(source, near)), sems)
    late = list(zip((state.at[layer], w_out.at[layer], gain), mix_near))
    if not layer:
        late += key_pairs(1, key_far, key_near)
    late = start_all(late, late_sems)
    for copy in copies:
        copy.wait()
    w_gate, w_value, w_step, bias, rate, skip, conv, taps = near
    hidden = scaled[...]
    inv_col = inv[:, :CH]
    gate = dot_nt(hidden, w_gate[...]) * inv_col
    fresh = dot_nt(hidden, w_value[...]) * inv_col
    step = jnp.dot(hidden, w_step[...], preferred_element_type=F32) * inv[...]
    old, newer = conv[:, 0, :], conv[:, 1, :]
    tap = [taps[k, layer : layer + 1, :] for k in range(3)]
    values = silu(old * tap[0] + newer * tap[1] + fresh * tap[2])
    if layer:
        conv_out[0] = before[0][...]
        conv_out[1, :, 0, :] = newer
        conv_out[1, :, 1, :] = fresh
    else:
        conv_out[:, 0, :] = newer
        conv_out[:, 1, :] = fresh
    head = lax.axis_index(("z", "y", "x"))
    mine = lax.broadcasted_iota(jnp.int32, (1, 128), 1) == head

    def of_head(table):
        return jnp.sum(jnp.where(mine, table, 0.0), axis=1, keepdims=True)

    raw = of_head(step + bias[layer : layer + 1, :])
    delta = jnp.maximum(raw, 0.0) + jnp.log1p(jnp.exp(-jnp.abs(raw)))
    decay = jnp.exp(-delta * of_head(rate[layer : layer + 1, :]))
    packed[0] = (delta * values).T
    packed[1] = of_head(skip[layer : layer + 1, :]) * values
    packed[2] = silu(gate)
    packed[3] = jnp.broadcast_to(decay, (B, CH))
    for copy in late:
        copy.wait()


def make_values(layer, scaled, inv, value_far, mix_far, key_far, before):
    near = [scaled, inv] + ([before] if layer else [])
    outs = [
        pltpu.VMEM((4, B, CH), F32),
        shaped((2, B, 2, CH), F32) if layer else pltpu.VMEM((B, 2, CH), F32),
    ]
    outs += [pltpu.VMEM(*p) for p in MIX_PARAMS]
    if not layer:
        outs += [pltpu.VMEM(*p) for p in KEY_PARAMS]
    else:
        key_far = []
    sems = [pltpu.SemaphoreType.DMA((8,)), pltpu.SemaphoreType.DMA((8,))]
    return call(
        functools.partial(values_kernel, layer),
        f"values{layer}",
        near,
        [*value_far, *mix_far, *key_far],
        outs,
        [pltpu.VMEM(*p) for p in VALUE_PARAMS] + sems,
    )


def mix_kernel(layer, keys, packed, state, w_out, gain, fresh, sent):
    both = (keys[0] + keys[1]).T
    writes, reads = both[:B], both[B : 2 * B]
    push = packed[0]
    decay = packed[3]
    lane = lax.broadcasted_iota(jnp.int32, (CH, B), 1)
    found = jnp.zeros((CH, B), F32)
    for b in range(B):
        new = decay[b : b + 1, :1] * state[b] + push[:, b : b + 1] * writes[b : b + 1]
        fresh[b] = new
        total = jnp.sum(new * reads[b : b + 1], axis=1, keepdims=True)
        found = jnp.where(lane == b, total, found)
    gated = (found.T + packed[1]) * packed[2]
    total = as_row(jnp.sum(gated * gated, axis=1, keepdims=True))
    high = total.astype(BF16).astype(F32)
    low = total - high
    row = lax.broadcasted_iota(jnp.int32, (8, B), 0)
    tail = jnp.where(row == 0, high, jnp.where(row == 1, low, 0.0))
    tail = jnp.concatenate([tail, jnp.zeros((8, 128 - B), F32)], axis=1).astype(BF16)
    out = jnp.dot((gated * gain[layer : layer + 1, :]).astype(BF16), w_out[...], preferred_element_type=F32)
    for j in range(D // 128):
        sent[j, :B] = out[:, 128 * j : 128 * j + 128].astype(BF16)
        sent[j, B:] = tail


def make_mix(layer, keys, packed, mix_near):
    return call(
        functools.partial(mix_kernel, layer),
        f"mix{layer}",
        [keys, packed, *mix_near],
        [],
        [pltpu.VMEM((B, CH, N), F32), pltpu.VMEM((32, 40, 128), BF16)],
    )


def scale_kernel(layer, got, fresh, *refs):
    sent, states, sem = refs[-3:]
    write_back = pltpu.make_async_copy(fresh, states.at[layer], sem)
    write_back.start()
    total = got[0].astype(F32)
    for j in range(1, 32):
        total += got[j].astype(F32)
    squares = total[B : B + 1, :B] + total[B + 1 : B + 2, :B]
    factor = as_col(lax.rsqrt(squares / GW + EPS))
    chunk = (total[:B] * factor).astype(BF16)
    for plane in range(8):
        sent[plane] = chunk
    write_back.wait()


def make_scale(layer, got, fresh, states):
    return call(
        functools.partial(scale_kernel, layer),
        f"scale{layer}",
        [got, fresh],
        [states] if layer else [],
        [pltpu.VMEM((8, B, 128), BF16), pltpu.HBM((2, B, CH, N), F32)],
        [pltpu.SemaphoreType.DMA],
        {2: 1} if layer else {},
    )


def add_kernel(layer, got, hid, sent):
    total = got[0].astype(F32)
    for plane in range(1, 8):
        total += got[plane].astype(F32)
    at = lax.axis_index(PLANE)
    if layer:
        own = hid[at]
    else:
        own = hid[:, pl.ds(pl.multiple_of(128 * at, 128), 128)]
    chunk = (own.astype(F32) + total).astype(BF16)
    for j in range(32):
        sent[j] = chunk


def make_add(layer, got, hid):
    return call(
        functools.partial(add_kernel, layer), f"add{layer}", [got, hid], [], [pltpu.VMEM((32, B, 128), BF16)]
    )[0]


def exchange(value, axes):
    return lax.all_to_all(value, axes, split_axis=0, concat_axis=0, tiled=True)


def per_device(
    tokens,
    norm_gain,
    w_gate,
    w_value,
    w_write,
    w_read,
    w_step,
    step_bias,
    decay_rate,
    skip_gain,
    conv_value_weight,
    conv_key_weight,
    group_gain,
    w_out,
    ssm_state,
    conv_value,
    conv_key,
):
    w_gate, w_value, w_write, w_read = (jnp.swapaxes(w, 1, 2) for w in (w_gate, w_value, w_write, w_read))
    conv_key = jnp.transpose(conv_key, (0, 2, 3, 4, 1))
    value_taps = jnp.swapaxes(conv_value_weight, 0, 1)
    key_far = [norm_gain, w_write, w_read, conv_key, conv_key_weight]
    value_far = [w_gate, w_value, w_step, step_bias, decay_rate, skip_gain, conv_value, value_taps]
    mix_far = [ssm_state, w_out, group_gain]
    states = value_out = None
    msg, key_out, scaled, inv, hid = first_keys(tokens, key_far)
    for layer in range(2):
        if layer:
            msg, key_out, scaled, inv = next_keys(hid, key_near, key_out)
        keys = exchange(msg.reshape(256, 128), ("c", "z", "y", "x")).reshape(2, 128, 128)
        packed, value_out, *near = make_values(layer, scaled, inv, value_far, mix_far, key_far, value_out)
        mix_near, key_near = near[:3], near[3:]
        fresh, sent = make_mix(layer, keys, packed, mix_near)
        sent, states = make_scale(layer, exchange(sent, PLANE), fresh, states)
        hid = exchange(make_add(layer, exchange(sent, ("z",)), hid), PLANE)
    tokens_out = jnp.transpose(hid, (1, 0, 2)).reshape(B, D)
    return (tokens_out, states, value_out, jnp.transpose(key_out, (0, 4, 1, 2, 3)))


def solution(mesh):
    torus = Mesh(mesh.devices.reshape(8, 4, 4, 2), TP)
    in_specs = (
        P(),
        P(),
        P(None, None, TP),
        P(None, None, TP),
        P(None, None, TP),
        P(None, None, TP),
        P(),
        P(),
        P(),
        P(),
        P(None, None, TP),
        P(None, None, None, TP),
        P(None, TP),
        P(None, TP, None),
        P(None, None, TP, None),
        P(None, None, None, TP),
        P(None, None, None, None, TP),
    )
    out_specs = (
        P(),
        P(None, None, TP, None),
        P(None, None, None, TP),
        P(None, None, None, None, TP),
    )
    return jax.shard_map(
        per_device, mesh=torus, in_specs=in_specs, out_specs=out_specs, check_vma=False
    )
```

```python
import functools

import jax
import jax.numpy as jnp
from jax import lax
from jax.experimental import pallas as pl
from jax.experimental.pallas import tpu as pltpu
from jax.sharding import Mesh
from jax.sharding import PartitionSpec as P

D = 4096
B = 32
CH = 32
N = 128
GW = 1024
EPS = 1e-06
TP = ("z", "y", "x", "c")
PLANE = ("y", "x", "c")
F32 = jnp.float32
BF16 = jnp.bfloat16


LIMIT = pltpu.CompilerParams(vmem_limit_bytes=8 * 1024 * 1024)


def vmem():
    return pl.BlockSpec(memory_space=pltpu.VMEM)


def anywhere():
    return pl.BlockSpec(memory_space=pl.ANY)


def shaped(shape, dtype):
    return jax.ShapeDtypeStruct(shape, dtype)


def start_all(pairs, sems):
    copies = [pltpu.make_async_copy(src, dst, sems.at[at]) for at, (src, dst) in enumerate(pairs)]
    for copy in copies:
        copy.start()
    return copies


def call(body, name, near, far, outs, scratch=(), aliases=None):
    near = [pltpu.with_memory_space_constraint(v, pltpu.VMEM) for v in near]
    far = [pltpu.with_memory_space_constraint(v, pltpu.HBM) for v in far]
    far_out = (pltpu.HBM((1,), F32).memory_space,)
    specs = [anywhere() if getattr(o, "memory_space", None) in far_out else vmem() for o in outs]
    return pl.pallas_call(
        body,
        in_specs=[vmem()] * len(near) + [anywhere()] * len(far),
        out_specs=specs,
        out_shape=list(outs),
        scratch_shapes=list(scratch),
        input_output_aliases=aliases or {},
        compiler_params=LIMIT,
        name=name,
    )(*near, *far)


def silu(v):
    return v / (1.0 + jnp.exp(-v))


def as_col(row):
    n = row.shape[1]
    at = lax.broadcasted_iota(jnp.int32, (n, n), 0)
    of = lax.broadcasted_iota(jnp.int32, (n, n), 1)
    return jnp.sum(jnp.where(at == of, row, 0.0), axis=1, keepdims=True)


def as_row(col):
    n = col.shape[0]
    at = lax.broadcasted_iota(jnp.int32, (n, n), 0)
    of = lax.broadcasted_iota(jnp.int32, (n, n), 1)
    return jnp.sum(jnp.where(at == of, col, 0.0), axis=0, keepdims=True)


def dot_nt(a, b):
    return lax.dot_general(a, b, (((1,), (1,)), ((), ())), preferred_element_type=F32)


def hi_lo(value):
    high = value.astype(BF16).astype(F32)
    return high, value - high


def scale_tokens(part_of, gain, scaled):
    squares = jnp.zeros((B, 128), F32)
    for j in range(D // 128):
        cols = slice(128 * j, 128 * j + 128)
        part = part_of(j).astype(F32)
        squares += part * part
        scaled[:, cols] = (part * gain[:, cols]).astype(BF16)
    return lax.rsqrt(jnp.sum(squares, axis=1, keepdims=True) / D + EPS)


KEY_WEIGHTS = ((4, D), BF16)


def keys_kernel(tokens, gain_far, write_far, read_far, conv_far, taps_far, msg, conv_out, scaled, inv_out, hid, *rest):
    gain, w_write, w_read, next_write, next_read, conv, taps, sems = rest
    pairs = [
        (tokens, hid),
        (gain_far, gain),
        (write_far.at[0], w_write),
        (read_far.at[0], w_read),
        (write_far.at[1], next_write),
        (read_far.at[1], next_read),
        (conv_far, conv),
        (taps_far, taps),
    ]
    for copy in start_all(pairs, sems):
        copy.wait()
    inv = scale_tokens(lambda j: hid[:, 128 * j : 128 * j + 128], gain.at[:1], scaled)
    inv_out[...] = jnp.broadcast_to(inv, (B, 128))
    inv_row = as_row(inv)
    mixed, later, last_taps = [], [], []
    for kind, weight in ((0, w_write), (1, w_read)):
        fresh = dot_nt(weight[...], scaled[...]) * inv_row
        old, newer = conv[0, 0, kind], conv[0, 1, kind]
        tap = [[as_col(taps[layer, k, kind : kind + 1, :]) for k in range(3)] for layer in range(2)]
        mixed.append(silu(old * tap[0][0] + newer * tap[0][1] + fresh * tap[0][2]))
        later.append(conv[1, 0, kind] * tap[1][0] + conv[1, 1, kind] * tap[1][1])
        last_taps.append(tap[1][2])
        conv_out[0, kind] = newer
        conv_out[1, kind] = fresh
    mixed_hi, mixed_lo = zip(*(hi_lo(v) for v in mixed))
    taps_hi, taps_lo = zip(*(hi_lo(v) for v in last_taps))
    first = jnp.concatenate([*mixed_hi, *later], axis=1)
    lane = lax.broadcasted_iota(jnp.int32, (4, B), 1)
    tail = jnp.zeros((4, B), F32)
    for at, col in enumerate((taps_hi[0], taps_lo[0], taps_hi[1], taps_lo[1])):
        tail = jnp.where(lane == at, col, tail)
    second = jnp.concatenate([*mixed_lo, tail, jnp.zeros((4, B), F32)], axis=1)
    row = lax.broadcasted_iota(jnp.int32, (4, 128), 0)
    for col in range(4):
        one = slice(col, col + 1)
        base = jnp.where(row == 2, first[one], second[one])
        for place in range(32):
            cols = slice(128 * place, 128 * place + 128)
            write = next_write[:, cols].astype(F32)[one]
            read = next_read[:, cols].astype(F32)[one]
            tile = jnp.where(row == 0, write, jnp.where(row == 1, read, base)).astype(BF16)
            at = 128 * (place % 2) + 16 * col + place // 2
            msg[at] = tile
            msg[at + 64] = tile


def make_keys(tokens, far):
    scratch = [((2, D), F32)] + [KEY_WEIGHTS] * 4 + [((2, 2, 2, 4, B), F32), ((2, 3, 2, 4), F32)]
    return call(
        keys_kernel,
        "keys",
        [],
        [tokens, *far],
        [
            shaped((256, 4, 128), BF16),
            pltpu.VMEM((2, 2, 4, B), F32),
            pltpu.VMEM((B, D), BF16),
            pltpu.VMEM((B, 128), F32),
            pltpu.VMEM((B, D), BF16),
        ],
        [pltpu.VMEM(*p) for p in scratch] + [pltpu.SemaphoreType.DMA((8,))],
    )


def of_head(table):
    head = lax.axis_index(("z", "y", "x"))
    mine = lax.broadcasted_iota(jnp.int32, (1, 128), 1) == head
    return jnp.sum(jnp.where(mine, table, 0.0), axis=1, keepdims=True)


def gated_values(layer, gate, fresh, raw, tables, conv, taps):
    bias, rate, skip = (t[layer : layer + 1, :] for t in tables)
    old, newer = conv[:, 0, :], conv[:, 1, :]
    tap = [taps[k, layer : layer + 1, :] for k in range(3)]
    values = silu(old * tap[0] + newer * tap[1] + fresh * tap[2])
    raw = raw + of_head(bias)
    delta = jnp.maximum(raw, 0.0) + jnp.log1p(jnp.exp(-jnp.abs(raw)))
    decay = jnp.exp(-delta * of_head(rate))
    return (delta * values).T, of_head(skip) * values, silu(gate), decay


STATE = ((B, CH, N), F32)
OUT = ((CH, D), BF16)
ROWS = 80
NOW_FAR = (((CH, D), BF16), ((CH, D), BF16), ((D, 128), BF16))
NEXT_FAR = (((D, 128), BF16), KEY_WEIGHTS, KEY_WEIGHTS)
KEPT = (
    STATE,
    OUT,
    ((2, CH), F32),
    STATE,
    OUT,
    ((2, D), F32),
    ((2, 128), F32),
    ((2, 128), F32),
    ((2, 128), F32),
    ((2, B, 2, CH), F32),
    ((3, 2, CH), F32),
    ((2, 2, 2, 4, B), F32),
)


def values_kernel(scaled, inv, *refs):
    far, refs = refs[:15], refs[15:]
    packed, conv_out, stack, *kept = refs[: 3 + len(KEPT)]
    w_gate, w_value, w_step, next_step, next_write, next_read, sems, late_sems = refs[3 + len(KEPT) :]
    gate_far, value_far, step_far, write_far, read_far, state_far, out_far, *tables_far = far
    tables_group, tables_rest = tables_far[0], tables_far[1:]
    late_sources = [
        state_far.at[0], out_far.at[0], tables_group, state_far.at[1], out_far.at[1], *tables_rest
    ]
    late = list(zip(late_sources, kept))
    small = [(src, dst) for src, dst in late[6:11]]
    now = [(gate_far.at[0], w_gate), (value_far.at[0], w_value), (step_far.at[0], w_step)] + small
    copies = start_all(now, sems)
    late = late[:6] + late[11:]
    late += [
        (gate_far.at[1], stack.at[:CH]),
        (value_far.at[1], stack.at[CH : 2 * CH]),
        (step_far.at[1], next_step),
        (write_far.at[1], next_write),
        (read_far.at[1], next_read),
    ]
    late = start_all(late, late_sems)
    for copy in copies:
        copy.wait()
    hidden = scaled[...]
    inv_col = inv[:, :CH]
    gate = dot_nt(hidden, w_gate[...]) * inv_col
    fresh = dot_nt(hidden, w_value[...]) * inv_col
    raw = of_head(jnp.dot(hidden, w_step[...], preferred_element_type=F32) * inv[...])
    tables, conv, taps = kept[6:9], kept[9], kept[10]
    push, direct, gate, decay = gated_values(0, gate, fresh, raw, tables, conv.at[0], taps)
    packed[0] = push
    packed[1] = direct
    packed[2] = gate
    packed[3] = jnp.broadcast_to(decay, (B, CH))
    conv_out[:, 0, :] = conv[0, :, 1, :]
    conv_out[:, 1, :] = fresh
    for copy in late:
        copy.wait()
    head = lax.axis_index(("z", "y", "x"))
    hot = (lax.broadcasted_iota(jnp.int32, (8, 128), 1) == head).astype(F32).astype(BF16)
    stack[2 * CH : 2 * CH + 8] = dot_nt(hot, next_step[...]).astype(BF16)
    both = jnp.concatenate([next_write[...].astype(F32), next_read[...].astype(F32)], axis=0)
    stack[2 * CH + 8 :] = both.astype(BF16)


def make_values(scaled, inv, far):
    outs = [pltpu.VMEM((4, B, CH), F32), pltpu.VMEM((B, 2, CH), F32), pltpu.VMEM((ROWS, D), BF16)]
    outs += [pltpu.VMEM(*p) for p in KEPT]
    scratch = [pltpu.VMEM(*p) for p in NOW_FAR + NEXT_FAR]
    scratch += [pltpu.SemaphoreType.DMA((8,)), pltpu.SemaphoreType.DMA((12,))]
    return call(values_kernel, "values", [scaled, inv], far, outs, scratch)


def advance(push, direct, gate, decay, writes, reads, state, w_out, gain, fresh, sent):
    lane = lax.broadcasted_iota(jnp.int32, (CH, B), 1)
    found = jnp.zeros((CH, B), F32)
    for b in range(B):
        new = decay[b : b + 1] * state[b] + push[:, b : b + 1] * writes[b : b + 1]
        fresh[b] = new
        total = jnp.sum(new * reads[b : b + 1], axis=1, keepdims=True)
        found = jnp.where(lane == b, total, found)
    gated = (found.T + direct) * gate
    total = as_row(jnp.sum(gated * gated, axis=1, keepdims=True))
    high, low = hi_lo(total)
    row = lax.broadcasted_iota(jnp.int32, (8, B), 0)
    tail = jnp.where(row == 0, high, jnp.where(row == 1, low, 0.0))
    tail = jnp.concatenate([tail, jnp.zeros((8, 128 - B), F32)], axis=1).astype(BF16)
    out = jnp.dot((gated * gain).astype(BF16), w_out[...], preferred_element_type=F32)
    for j in range(D // 128):
        sent[j, :B] = out[:, 128 * j : 128 * j + 128].astype(BF16)
        sent[j, B:] = tail


PLANE_SUMS = ((32, B + 8, 128), BF16)


def first_mix_kernel(keys, packed, state, w_out, gain, fresh, sent, weights, later, last_taps, lines):
    lines[...] = keys[lax.axis_index("z") // 4].astype(F32)
    weights[0] = lines[pl.ds(0, N, stride=4), :].astype(BF16)
    weights[1] = lines[pl.ds(1, N, stride=4), :].astype(BF16)
    first = lines[pl.ds(2, N, stride=4), :].T
    second = lines[pl.ds(3, N, stride=4), :].T
    later[0] = first[2 * B : 3 * B]
    later[1] = first[3 * B :]
    last_taps[...] = second[2 * B : 2 * B + 8]
    writes = first[:B] + second[:B]
    reads = first[B : 2 * B] + second[B : 2 * B]
    advance(
        packed[0], packed[1], packed[2], packed[3][:, :1], writes, reads, state, w_out, gain[:1, :], fresh, sent
    )


def first_mix(keys, packed, kept):
    return call(
        first_mix_kernel,
        "mix0",
        [keys, packed, *kept],
        [],
        [
            pltpu.VMEM(*STATE),
            pltpu.VMEM(*PLANE_SUMS),
            pltpu.VMEM((2, N, 128), BF16),
            pltpu.VMEM((2, B, N), F32),
            pltpu.VMEM((8, N), F32),
        ],
        [pltpu.VMEM((4 * N, 128), F32)],
    )


def next_mix_kernel(own, other, stack, later, last_taps, state, w_out, gain, norm_gain, *refs):
    tables, conv, taps, key_conv, key_before, value_before = refs[:3], refs[3], refs[4], refs[5], refs[6], refs[7]
    fresh, sent, key_out, value_out, hid, scaled = refs[8:]
    core = lax.axis_index("c")
    sums = [jnp.zeros((B, N), F32), jnp.zeros((B, N), F32)]
    for at in range(16):
        for whose, side in ((own, core), (other, 1 - core)):
            hid[2 * at + side] = whose[at, :B]
            for kind in range(2):
                sums[kind] += whose[at, B * (kind + 1) : B * (kind + 2)].astype(F32)
    inv = scale_tokens(lambda j: hid[j], norm_gain.at[1:], scaled)
    found = dot_nt(scaled[...], stack[...]) * inv
    keys = [silu(later[k] + sums[k] * inv * (last_taps[2 * k : 2 * k + 1] + last_taps[2 * k + 1 : 2 * k + 2])) for k in range(2)]
    fresh_values = found[:, CH : 2 * CH]
    push, direct, gate, decay = gated_values(
        1, found[:, :CH], fresh_values, found[:, 2 * CH : 2 * CH + 1], tables, conv.at[1], taps
    )
    advance(push, direct, gate, decay, keys[0], keys[1], state, w_out, gain[1:, :], fresh, sent)
    value_out[0] = value_before[...]
    value_out[1, :, 0, :] = conv[1, :, 1, :]
    value_out[1, :, 1, :] = fresh_values
    turned = found.T
    key_out[0] = key_before[...]
    for kind in range(2):
        key_out[1, 0, kind] = key_conv[1, 1, kind]
        key_out[1, 1, kind] = turned[2 * CH + 8 + 4 * kind : 2 * CH + 12 + 4 * kind]


def next_mix(own, other, stack, later, last_taps, kept, key_before, value_before):
    return call(
        next_mix_kernel,
        "mix1",
        [own, other, stack, later, last_taps, *kept, key_before, value_before],
        [],
        [
            pltpu.VMEM(*STATE),
            pltpu.VMEM(*PLANE_SUMS),
            shaped((2, 2, 2, 4, B), F32),
            shaped((2, B, 2, CH), F32),
        ],
        [pltpu.VMEM((32, B, 128), BF16), pltpu.VMEM((B, D), BF16)],
    )


def scale_kernel(layer, got, fresh, *refs):
    sent, states, sem = refs[-3:]
    write_back = pltpu.make_async_copy(fresh, states.at[layer], sem)
    write_back.start()
    total = got[0].astype(F32)
    for j in range(1, 32):
        total += got[j].astype(F32)
    squares = total[B : B + 1, :B] + total[B + 1 : B + 2, :B]
    factor = as_col(lax.rsqrt(squares / GW + EPS))
    chunk = (total[:B] * factor).astype(BF16)
    for plane in range(8):
        sent[plane] = chunk
    write_back.wait()


def make_scale(layer, got, fresh, states):
    return call(
        functools.partial(scale_kernel, layer),
        f"scale{layer}",
        [got, fresh],
        [states] if layer else [],
        [pltpu.VMEM((8, B, 128), BF16), pltpu.HBM((2, B, CH, N), F32)],
        [pltpu.SemaphoreType.DMA],
        {2: 1} if layer else {},
    )


def first_add_kernel(got, hid, norm_gain, weights, sent):
    total = got[0].astype(F32)
    for plane in range(1, 8):
        total += got[plane].astype(F32)
    cols = pl.ds(pl.multiple_of(128 * lax.axis_index(PLANE), 128), 128)
    chunk = (hid[:, cols].astype(F32) + total).astype(BF16)
    scaled = (chunk.astype(F32) * norm_gain[1:, cols]).astype(BF16)
    shares = [dot_nt(scaled, weights[kind]).astype(BF16) for kind in range(2)]
    for j in range(16):
        sent[j, :B] = chunk
        sent[j, B : 2 * B] = shares[0]
        sent[j, 2 * B :] = shares[1]


def next_add_kernel(got, hid, sent):
    total = got[0].astype(F32)
    for plane in range(1, 8):
        total += got[plane].astype(F32)
    chunk = (hid[lax.axis_index(("y", "x")), :B].astype(F32) + total).astype(BF16)
    for j in range(32):
        sent[j] = chunk


def exchange(value, axes):
    return lax.all_to_all(value, axes, split_axis=0, concat_axis=0, tiled=True)


def per_device(
    tokens,
    norm_gain,
    w_gate,
    w_value,
    w_write,
    w_read,
    w_step,
    step_bias,
    decay_rate,
    skip_gain,
    conv_value_weight,
    conv_key_weight,
    group_gain,
    w_out,
    ssm_state,
    conv_value,
    conv_key,
):
    w_gate, w_value, w_write, w_read = (jnp.swapaxes(w, 1, 2) for w in (w_gate, w_value, w_write, w_read))
    conv_key = jnp.transpose(conv_key, (0, 2, 3, 4, 1))
    value_taps = jnp.swapaxes(conv_value_weight, 0, 1)
    far = [w_gate, w_value, w_step, w_write, w_read, ssm_state, w_out, group_gain, norm_gain]
    far += [step_bias, decay_rate, skip_gain, conv_value, value_taps, conv_key]
    msg, key_out, scaled, inv, hid = make_keys(tokens, [norm_gain, w_write, w_read, conv_key, conv_key_weight])
    keys = exchange(msg, ("c", "z", "y", "x")).reshape(2, 4 * N, 128)
    packed, value_out, stack, *kept = make_values(scaled, inv, far)
    state, out, gain, next_state, next_out, *rest = kept
    fresh, sent, weights, later, last_taps = first_mix(keys, packed, [state, out, gain])
    sent, states = make_scale(0, exchange(sent, PLANE), fresh, None)
    (sent,) = call(
        first_add_kernel,
        "add0",
        [exchange(sent, ("z",)), hid, rest[0], weights],
        [],
        [pltpu.VMEM((16, 3 * B, 128), BF16)],
    )
    own = exchange(sent, ("y", "x"))
    other = lax.ppermute(own, "c", [(0, 1), (1, 0)])
    fresh, sent, key_out, value_out = next_mix(
        own, other, stack, later, last_taps, [next_state, next_out, gain, *rest], key_out, value_out
    )
    sent, states = make_scale(1, exchange(sent, PLANE), fresh, states)
    (sent,) = call(next_add_kernel, "add1", [exchange(sent, ("z",)), own], [], [pltpu.VMEM((32, B, 128), BF16)])
    hid = exchange(sent, PLANE)
    tokens_out = jnp.transpose(hid, (1, 0, 2)).reshape(B, D)
    return (tokens_out, states, value_out, jnp.transpose(key_out, (0, 4, 1, 2, 3)))


def solution(mesh):
    torus = Mesh(mesh.devices.reshape(8, 4, 4, 2), TP)
    in_specs = (
        P(),
        P(),
        P(None, None, TP),
        P(None, None, TP),
        P(None, None, TP),
        P(None, None, TP),
        P(),
        P(),
        P(),
        P(),
        P(None, None, TP),
        P(None, None, None, TP),
        P(None, TP),
        P(None, TP, None),
        P(None, None, TP, None),
        P(None, None, None, TP),
        P(None, None, None, None, TP),
    )
    out_specs = (
        P(),
        P(None, None, TP, None),
        P(None, None, None, TP),
        P(None, None, None, None, TP),
    )
    return jax.shard_map(
        per_device, mesh=torus, in_specs=in_specs, out_specs=out_specs, check_vma=False
    )
```

```python
import functools

import jax
import jax.numpy as jnp
from jax import lax
from jax.experimental import pallas as pl
from jax.experimental.pallas import tpu as pltpu
from jax.sharding import Mesh
from jax.sharding import PartitionSpec as P

D = 4096
B = 32
CH = 32
N = 128
GW = 1024
EPS = 1e-06
TP = ("z", "y", "x", "c")
PLANE = ("y", "x", "c")
F32 = jnp.float32
BF16 = jnp.bfloat16


LIMIT = pltpu.CompilerParams(vmem_limit_bytes=8 * 1024 * 1024)


def vmem():
    return pl.BlockSpec(memory_space=pltpu.VMEM)


def anywhere():
    return pl.BlockSpec(memory_space=pl.ANY)


def shaped(shape, dtype):
    return jax.ShapeDtypeStruct(shape, dtype)


def start_all(pairs, sems):
    copies = [pltpu.make_async_copy(src, dst, sems.at[at]) for at, (src, dst) in enumerate(pairs)]
    for copy in copies:
        copy.start()
    return copies


def call(body, name, near, far, outs, scratch=(), aliases=None):
    near = [pltpu.with_memory_space_constraint(v, pltpu.VMEM) for v in near]
    far = [pltpu.with_memory_space_constraint(v, pltpu.HBM) for v in far]
    far_out = (pltpu.HBM((1,), F32).memory_space,)
    specs = [anywhere() if getattr(o, "memory_space", None) in far_out else vmem() for o in outs]
    return pl.pallas_call(
        body,
        in_specs=[vmem()] * len(near) + [anywhere()] * len(far),
        out_specs=specs,
        out_shape=list(outs),
        scratch_shapes=list(scratch),
        input_output_aliases=aliases or {},
        compiler_params=LIMIT,
        name=name,
    )(*near, *far)


def silu(v):
    return v / (1.0 + jnp.exp(-v))


def as_col(row):
    n = row.shape[1]
    at = lax.broadcasted_iota(jnp.int32, (n, n), 0)
    of = lax.broadcasted_iota(jnp.int32, (n, n), 1)
    return jnp.sum(jnp.where(at == of, row, 0.0), axis=1, keepdims=True)


def as_row(col):
    n = col.shape[0]
    at = lax.broadcasted_iota(jnp.int32, (n, n), 0)
    of = lax.broadcasted_iota(jnp.int32, (n, n), 1)
    return jnp.sum(jnp.where(at == of, col, 0.0), axis=0, keepdims=True)


def dot_nt(a, b):
    return lax.dot_general(a, b, (((1,), (1,)), ((), ())), preferred_element_type=F32)


def hi_lo(value):
    high = value.astype(BF16).astype(F32)
    return high, value - high


def scale_tokens(part_of, gain, scaled):
    squares = jnp.zeros((B, 128), F32)
    for j in range(D // 128):
        cols = slice(128 * j, 128 * j + 128)
        part = part_of(j).astype(F32)
        squares += part * part
        scaled[:, cols] = (part * gain[:, cols]).astype(BF16)
    return lax.rsqrt(jnp.sum(squares, axis=1, keepdims=True) / D + EPS)


KEY_WEIGHTS = ((4, D), BF16)


def keys_kernel(tokens, gain_far, write_far, read_far, conv_far, taps_far, msg, conv_out, scaled, inv_out, hid, *rest):
    gain, w_write, w_read, next_write, next_read, conv, taps, sems = rest
    pairs = [
        (tokens, hid),
        (gain_far, gain),
        (write_far.at[0], w_write),
        (read_far.at[0], w_read),
        (write_far.at[1], next_write),
        (read_far.at[1], next_read),
        (conv_far, conv),
        (taps_far, taps),
    ]
    for copy in start_all(pairs, sems):
        copy.wait()
    inv = scale_tokens(lambda j: hid[:, 128 * j : 128 * j + 128], gain.at[:1], scaled)
    inv_out[...] = jnp.broadcast_to(inv, (B, 128))
    inv_row = as_row(inv)
    mixed, later, last_taps = [], [], []
    for kind, weight in ((0, w_write), (1, w_read)):
        fresh = dot_nt(weight[...], scaled[...]) * inv_row
        old, newer = conv[0, 0, kind], conv[0, 1, kind]
        tap = [[as_col(taps[layer, k, kind : kind + 1, :]) for k in range(3)] for layer in range(2)]
        mixed.append(silu(old * tap[0][0] + newer * tap[0][1] + fresh * tap[0][2]))
        later.append(conv[1, 0, kind] * tap[1][0] + conv[1, 1, kind] * tap[1][1])
        last_taps.append(tap[1][2])
        conv_out[0, kind] = newer
        conv_out[1, kind] = fresh
    mixed_hi, mixed_lo = zip(*(hi_lo(v) for v in mixed))
    taps_hi, taps_lo = zip(*(hi_lo(v) for v in last_taps))
    first = jnp.concatenate([*mixed_hi, *later], axis=1)
    lane = lax.broadcasted_iota(jnp.int32, (4, B), 1)
    tail = jnp.zeros((4, B), F32)
    for at, col in enumerate((taps_hi[0], taps_lo[0], taps_hi[1], taps_lo[1])):
        tail = jnp.where(lane == at, col, tail)
    second = jnp.concatenate([*mixed_lo, tail, jnp.zeros((4, B), F32)], axis=1)
    row = lax.broadcasted_iota(jnp.int32, (4, 128), 0)
    for col in range(4):
        one = slice(col, col + 1)
        base = jnp.where(row == 2, first[one], second[one])
        for place in range(32):
            cols = slice(128 * place, 128 * place + 128)
            write = next_write[:, cols].astype(F32)[one]
            read = next_read[:, cols].astype(F32)[one]
            tile = jnp.where(row == 0, write, jnp.where(row == 1, read, base)).astype(BF16)
            at = 128 * (place % 2) + 16 * col + place // 2
            msg[at] = tile
            msg[at + 64] = tile


def make_keys(tokens, far):
    scratch = [((2, D), F32)] + [KEY_WEIGHTS] * 4 + [((2, 2, 2, 4, B), F32), ((2, 3, 2, 4), F32)]
    return call(
        keys_kernel,
        "keys",
        [],
        [tokens, *far],
        [
            shaped((256, 4, 128), BF16),
            pltpu.VMEM((2, 2, 4, B), F32),
            pltpu.VMEM((B, D), BF16),
            pltpu.VMEM((B, 128), F32),
            pltpu.VMEM((B, D), BF16),
        ],
        [pltpu.VMEM(*p) for p in scratch] + [pltpu.SemaphoreType.DMA((8,))],
    )


def of_head(table):
    head = lax.axis_index(("z", "y", "x"))
    mine = lax.broadcasted_iota(jnp.int32, (1, 128), 1) == head
    return jnp.sum(jnp.where(mine, table, 0.0), axis=1, keepdims=True)


def gated_values(layer, gate, fresh, raw, tables, conv, taps):
    bias, rate, skip = (t[layer : layer + 1, :] for t in tables)
    old, newer = conv[:, 0, :], conv[:, 1, :]
    tap = [taps[k, layer : layer + 1, :] for k in range(3)]
    values = silu(old * tap[0] + newer * tap[1] + fresh * tap[2])
    raw = raw + of_head(bias)
    delta = jnp.maximum(raw, 0.0) + jnp.log1p(jnp.exp(-jnp.abs(raw)))
    decay = jnp.exp(-delta * of_head(rate))
    return (delta * values).T, of_head(skip) * values, silu(gate), decay


STATE = ((B, CH, N), F32)
OUT = ((CH, D), BF16)
ROWS = 80
NOW_FAR = (((CH, D), BF16), ((CH, D), BF16), ((D, 128), BF16))
NEXT_FAR = (((D, 128), BF16), KEY_WEIGHTS, KEY_WEIGHTS)
KEPT = (
    STATE,
    OUT,
    ((2, CH), F32),
    STATE,
    OUT,
    ((2, D), F32),
    ((2, 128), F32),
    ((2, 128), F32),
    ((2, 128), F32),
    ((2, B, 2, CH), F32),
    ((3, 2, CH), F32),
    ((2, 2, 2, 4, B), F32),
)


def values_kernel(scaled, inv, *refs):
    far, refs = refs[:15], refs[15:]
    packed, decay_out, conv_out, stack, *kept = refs[: 4 + len(KEPT)]
    w_gate, w_value, w_step, next_step, next_write, next_read, sems, late_sems = refs[4 + len(KEPT) :]
    gate_far, value_far, step_far, write_far, read_far, state_far, out_far, *tables_far = far
    tables_group, tables_rest = tables_far[0], tables_far[1:]
    late_sources = [
        state_far.at[0], out_far.at[0], tables_group, state_far.at[1], out_far.at[1], *tables_rest
    ]
    late = list(zip(late_sources, kept))
    small = [(src, dst) for src, dst in late[6:11]]
    now = [(gate_far.at[0], w_gate), (value_far.at[0], w_value), (step_far.at[0], w_step)] + small
    copies = start_all(now, sems)
    late = late[:6] + late[11:]
    late += [
        (gate_far.at[1], stack.at[:CH]),
        (value_far.at[1], stack.at[CH : 2 * CH]),
        (step_far.at[1], next_step),
        (write_far.at[1], next_write),
        (read_far.at[1], next_read),
    ]
    late = start_all(late, late_sems)
    for copy in copies:
        copy.wait()
    hidden = scaled[...]
    inv_col = inv[:, :CH]
    gate = dot_nt(hidden, w_gate[...]) * inv_col
    fresh = dot_nt(hidden, w_value[...]) * inv_col
    raw = of_head(jnp.dot(hidden, w_step[...], preferred_element_type=F32) * inv[...])
    tables, conv, taps = kept[6:9], kept[9], kept[10]
    push, direct, gate, decay = gated_values(0, gate, fresh, raw, tables, conv.at[0], taps)
    packed[0] = push
    packed[1] = direct
    packed[2] = gate
    decay_out[...] = jnp.broadcast_to(decay, (B, N))
    conv_out[:, 0, :] = conv[0, :, 1, :]
    conv_out[:, 1, :] = fresh
    for copy in late:
        copy.wait()
    head = lax.axis_index(("z", "y", "x"))
    hot = (lax.broadcasted_iota(jnp.int32, (8, 128), 1) == head).astype(F32).astype(BF16)
    stack[2 * CH : 2 * CH + 8] = dot_nt(hot, next_step[...]).astype(BF16)
    both = jnp.concatenate([next_write[...].astype(F32), next_read[...].astype(F32)], axis=0)
    stack[2 * CH + 8 :] = both.astype(BF16)


def make_values(scaled, inv, far):
    outs = [pltpu.VMEM((3, B, CH), F32), pltpu.VMEM((B, N), F32)]
    outs += [pltpu.VMEM((B, 2, CH), F32), pltpu.VMEM((ROWS, D), BF16)]
    outs += [pltpu.VMEM(*p) for p in KEPT]
    scratch = [pltpu.VMEM(*p) for p in NOW_FAR + NEXT_FAR]
    scratch += [pltpu.SemaphoreType.DMA((8,)), pltpu.SemaphoreType.DMA((12,))]
    return call(values_kernel, "values", [scaled, inv], far, outs, scratch)


def advance(layer, push, direct, gate, writes, reads, state, w_out, gain, sent, states, scratch):
    fresh, decay_rows, read_rows, sems = scratch
    read_rows[...] = reads
    high, low = hi_lo(push)
    left = jnp.concatenate([high, high, low], axis=1)
    high, low = hi_lo(writes)
    right = jnp.concatenate([high, low, high], axis=0).astype(BF16)
    of = lax.broadcasted_iota(jnp.int32, left.shape, 1) % B
    left = jnp.concatenate([jnp.where(of == b, left, 0.0).astype(BF16) for b in range(B)], axis=0)
    pushed = jnp.dot(left, right, preferred_element_type=F32)
    lane = lax.broadcasted_iota(jnp.int32, (CH, B), 1)
    found = jnp.zeros((CH, B), F32)
    copies = []
    for b in range(B):
        new = decay_rows[b : b + 1, :] * state[b] + pushed[CH * b : CH * (b + 1)]
        fresh[b] = new
        total = jnp.sum(new * read_rows[b : b + 1, :], axis=1, keepdims=True)
        found = jnp.where(lane == b, total, found)
        if b % 8 == 7:
            part = pl.ds(b - 7, 8)
            copies.append(pltpu.make_async_copy(fresh.at[part], states.at[layer, part], sems.at[b // 8]))
            copies[-1].start()
    gated = (found.T + direct) * gate
    total = as_row(jnp.sum(gated * gated, axis=1, keepdims=True))
    high, low = hi_lo(total)
    row = lax.broadcasted_iota(jnp.int32, (8, B), 0)
    tail = jnp.where(row == 0, high, jnp.where(row == 1, low, 0.0))
    tail = jnp.concatenate([tail, jnp.zeros((8, 128 - B), F32)], axis=1).astype(BF16)
    out = jnp.dot((gated * gain).astype(BF16), w_out[...], preferred_element_type=F32)
    for j in range(D // 128):
        sent[j, :B] = out[:, 128 * j : 128 * j + 128].astype(BF16)
        sent[j, B:] = tail
    for copy in copies:
        copy.wait()


STATES = ((2, B, CH, N), F32)
ADVANCE = (STATE, ((B, N), F32), ((B, N), F32))


def advance_scratch():
    return [pltpu.VMEM(*p) for p in ADVANCE] + [pltpu.SemaphoreType.DMA((4,))]


PLANE_SUMS = ((32, B + 8, 128), BF16)


def first_mix_kernel(keys, packed, decay, state, w_out, gain, states, sent, weights, later, last_taps, lines, *scratch):
    lines[...] = keys[lax.axis_index("z") // 4].astype(F32)
    weights[0] = lines[pl.ds(0, N, stride=4), :].astype(BF16)
    weights[1] = lines[pl.ds(1, N, stride=4), :].astype(BF16)
    first = lines[pl.ds(2, N, stride=4), :].T
    second = lines[pl.ds(3, N, stride=4), :].T
    later[0] = first[2 * B : 3 * B]
    later[1] = first[3 * B :]
    last_taps[...] = second[2 * B : 2 * B + 8]
    writes = first[:B] + second[:B]
    reads = first[B : 2 * B] + second[B : 2 * B]
    scratch[1][...] = decay[...]
    advance(
        0, packed[0], packed[1], packed[2], writes, reads, state, w_out, gain[:1, :], sent, states, scratch
    )


def first_mix(keys, packed, decay, kept):
    return call(
        first_mix_kernel,
        "mix0",
        [keys, packed, decay, *kept],
        [],
        [
            pltpu.HBM(*STATES),
            pltpu.VMEM(*PLANE_SUMS),
            pltpu.VMEM((2, N, 128), BF16),
            pltpu.VMEM((2, B, N), F32),
            pltpu.VMEM((8, N), F32),
        ],
        [pltpu.VMEM((4 * N, 128), F32)] + advance_scratch(),
    )


def next_mix_kernel(own, other, stack, later, last_taps, state, w_out, gain, norm_gain, *refs):
    tables, conv, taps, key_conv, key_before, value_before = refs[:3], refs[3], refs[4], refs[5], refs[6], refs[7]
    states, sent, key_out, value_out, hid, scaled, *scratch = refs[9:]
    core = lax.axis_index("c")
    sums = [jnp.zeros((B, N), F32), jnp.zeros((B, N), F32)]
    for at in range(16):
        for whose, side in ((own, core), (other, 1 - core)):
            hid[2 * at + side] = whose[at, :B]
            for kind in range(2):
                sums[kind] += whose[at, B * (kind + 1) : B * (kind + 2)].astype(F32)
    inv = scale_tokens(lambda j: hid[j], norm_gain.at[1:], scaled)
    found = dot_nt(scaled[...], stack[...]) * inv
    keys = [silu(later[k] + sums[k] * inv * (last_taps[2 * k : 2 * k + 1] + last_taps[2 * k + 1 : 2 * k + 2])) for k in range(2)]
    fresh_values = found[:, CH : 2 * CH]
    push, direct, gate, decay = gated_values(
        1, found[:, :CH], fresh_values, found[:, 2 * CH : 2 * CH + 1], tables, conv.at[1], taps
    )
    scratch[1][...] = jnp.broadcast_to(decay, (B, N))
    advance(1, push, direct, gate, keys[0], keys[1], state, w_out, gain[1:, :], sent, states, scratch)
    value_out[0] = value_before[...]
    value_out[1, :, 0, :] = conv[1, :, 1, :]
    value_out[1, :, 1, :] = fresh_values
    turned = found.T
    key_out[0] = key_before[...]
    for kind in range(2):
        key_out[1, 0, kind] = key_conv[1, 1, kind]
        key_out[1, 1, kind] = turned[2 * CH + 8 + 4 * kind : 2 * CH + 12 + 4 * kind]


def next_mix(own, other, stack, later, last_taps, kept, key_before, value_before, states):
    return call(
        next_mix_kernel,
        "mix1",
        [own, other, stack, later, last_taps, *kept, key_before, value_before],
        [states],
        [
            pltpu.HBM(*STATES),
            pltpu.VMEM(*PLANE_SUMS),
            shaped((2, 2, 2, 4, B), F32),
            shaped((2, B, 2, CH), F32),
        ],
        [pltpu.VMEM((32, B, 128), BF16), pltpu.VMEM((B, D), BF16)] + advance_scratch(),
        {17: 0},
    )


def scale_kernel(got, sent):
    total = got[0].astype(F32)
    for j in range(1, 32):
        total += got[j].astype(F32)
    squares = total[B : B + 1, :B] + total[B + 1 : B + 2, :B]
    factor = as_col(lax.rsqrt(squares / GW + EPS))
    chunk = (total[:B] * factor).astype(BF16)
    for plane in range(8):
        sent[plane] = chunk


def make_scale(got):
    return call(scale_kernel, "scale", [got], [], [pltpu.VMEM((8, B, 128), BF16)])[0]


def first_add_kernel(got, hid, norm_gain, weights, sent):
    total = got[0].astype(F32)
    for plane in range(1, 8):
        total += got[plane].astype(F32)
    cols = pl.ds(pl.multiple_of(128 * lax.axis_index(PLANE), 128), 128)
    chunk = (hid[:, cols].astype(F32) + total).astype(BF16)
    scaled = (chunk.astype(F32) * norm_gain[1:, cols]).astype(BF16)
    shares = [dot_nt(scaled, weights[kind]).astype(BF16) for kind in range(2)]
    for j in range(16):
        sent[j, :B] = chunk
        sent[j, B : 2 * B] = shares[0]
        sent[j, 2 * B :] = shares[1]


def next_add_kernel(got, hid, sent):
    total = got[0].astype(F32)
    for plane in range(1, 8):
        total += got[plane].astype(F32)
    chunk = (hid[lax.axis_index(("y", "x")), :B].astype(F32) + total).astype(BF16)
    for j in range(32):
        sent[j] = chunk


def exchange(value, axes):
    return lax.all_to_all(value, axes, split_axis=0, concat_axis=0, tiled=True)


def per_device(
    tokens,
    norm_gain,
    w_gate,
    w_value,
    w_write,
    w_read,
    w_step,
    step_bias,
    decay_rate,
    skip_gain,
    conv_value_weight,
    conv_key_weight,
    group_gain,
    w_out,
    ssm_state,
    conv_value,
    conv_key,
):
    w_gate, w_value, w_write, w_read = (jnp.swapaxes(w, 1, 2) for w in (w_gate, w_value, w_write, w_read))
    conv_key = jnp.transpose(conv_key, (0, 2, 3, 4, 1))
    value_taps = jnp.swapaxes(conv_value_weight, 0, 1)
    far = [w_gate, w_value, w_step, w_write, w_read, ssm_state, w_out, group_gain, norm_gain]
    far += [step_bias, decay_rate, skip_gain, conv_value, value_taps, conv_key]
    msg, key_out, scaled, inv, hid = make_keys(tokens, [norm_gain, w_write, w_read, conv_key, conv_key_weight])
    keys = exchange(msg, ("c", "z", "y", "x")).reshape(2, 4 * N, 128)
    packed, decay, value_out, stack, *kept = make_values(scaled, inv, far)
    state, out, gain, next_state, next_out, *rest = kept
    states, sent, weights, later, last_taps = first_mix(keys, packed, decay, [state, out, gain])
    sent = make_scale(exchange(sent, PLANE))
    (sent,) = call(
        first_add_kernel,
        "add0",
        [exchange(sent, ("z",)), hid, rest[0], weights],
        [],
        [pltpu.VMEM((16, 3 * B, 128), BF16)],
    )
    own = exchange(sent, ("y", "x"))
    other = lax.ppermute(own, "c", [(0, 1), (1, 0)])
    states, sent, key_out, value_out = next_mix(
        own, other, stack, later, last_taps, [next_state, next_out, gain, *rest], key_out, value_out, states
    )
    sent = make_scale(exchange(sent, PLANE))
    (sent,) = call(next_add_kernel, "add1", [exchange(sent, ("z",)), own], [], [pltpu.VMEM((32, B, 128), BF16)])
    hid = exchange(sent, PLANE)
    tokens_out = jnp.transpose(hid, (1, 0, 2)).reshape(B, D)
    return (tokens_out, states, value_out, jnp.transpose(key_out, (0, 4, 1, 2, 3)))


def solution(mesh):
    torus = Mesh(mesh.devices.reshape(8, 4, 4, 2), TP)
    in_specs = (
        P(),
        P(),
        P(None, None, TP),
        P(None, None, TP),
        P(None, None, TP),
        P(None, None, TP),
        P(),
        P(),
        P(),
        P(),
        P(None, None, TP),
        P(None, None, None, TP),
        P(None, TP),
        P(None, TP, None),
        P(None, None, TP, None),
        P(None, None, None, TP),
        P(None, None, None, None, TP),
    )
    out_specs = (
        P(),
        P(None, None, TP, None),
        P(None, None, None, TP),
        P(None, None, None, None, TP),
    )
    return jax.shard_map(
        per_device, mesh=torus, in_specs=in_specs, out_specs=out_specs, check_vma=False
    )
```

```python
import functools

import jax
import jax.numpy as jnp
from jax import lax
from jax.experimental import pallas as pl
from jax.experimental.pallas import tpu as pltpu
from jax.sharding import Mesh
from jax.sharding import PartitionSpec as P

D = 4096
B = 32
CH = 32
N = 128
GW = 1024
LINES = B + 2
EPS = 1e-06
TP = ("z", "y", "x", "c")
PLANE = ("y", "x", "c")
F32 = jnp.float32
BF16 = jnp.bfloat16


LIMIT = pltpu.CompilerParams(vmem_limit_bytes=8 * 1024 * 1024)


def vmem():
    return pl.BlockSpec(memory_space=pltpu.VMEM)


def anywhere():
    return pl.BlockSpec(memory_space=pl.ANY)


def shaped(shape, dtype):
    return jax.ShapeDtypeStruct(shape, dtype)


def start_all(pairs, sems):
    copies = [pltpu.make_async_copy(src, dst, sems.at[at]) for at, (src, dst) in enumerate(pairs)]
    for copy in copies:
        copy.start()
    return copies


def call(body, name, near, far, outs, scratch=(), aliases=None):
    near = [pltpu.with_memory_space_constraint(v, pltpu.VMEM) for v in near]
    far = [pltpu.with_memory_space_constraint(v, pltpu.HBM) for v in far]
    far_out = (pltpu.HBM((1,), F32).memory_space,)
    specs = [anywhere() if getattr(o, "memory_space", None) in far_out else vmem() for o in outs]
    return pl.pallas_call(
        body,
        in_specs=[vmem()] * len(near) + [anywhere()] * len(far),
        out_specs=specs,
        out_shape=list(outs),
        scratch_shapes=list(scratch),
        input_output_aliases=aliases or {},
        compiler_params=LIMIT,
        name=name,
    )(*near, *far)


def silu(v):
    return v / (1.0 + jnp.exp(-v))


def as_col(row):
    n = row.shape[1]
    at = lax.broadcasted_iota(jnp.int32, (n, n), 0)
    of = lax.broadcasted_iota(jnp.int32, (n, n), 1)
    return jnp.sum(jnp.where(at == of, row, 0.0), axis=1, keepdims=True)


def as_row(col):
    n = col.shape[0]
    at = lax.broadcasted_iota(jnp.int32, (n, n), 0)
    of = lax.broadcasted_iota(jnp.int32, (n, n), 1)
    return jnp.sum(jnp.where(at == of, col, 0.0), axis=0, keepdims=True)


def dot_nt(a, b):
    return lax.dot_general(a, b, (((1,), (1,)), ((), ())), preferred_element_type=F32)


def hi_lo(value):
    high = value.astype(BF16).astype(F32)
    return high, value - high


def scale_tokens(part_of, gain, scaled):
    squares = jnp.zeros((B, 128), F32)
    for j in range(D // 128):
        cols = slice(128 * j, 128 * j + 128)
        part = part_of(j).astype(F32)
        squares += part * part
        scaled[:, cols] = (part * gain[:, cols]).astype(BF16)
    return lax.rsqrt(jnp.sum(squares, axis=1, keepdims=True) / D + EPS)


KEY_WEIGHTS = ((4, D), BF16)


def keys_kernel(tokens, gain_far, write_far, read_far, conv_far, taps_far, msg, conv_out, scaled, inv_out, hid, *rest):
    gain, w_write, w_read, next_write, next_read, conv, taps, sems = rest
    pairs = [
        (tokens, hid),
        (gain_far, gain),
        (write_far.at[0], w_write),
        (read_far.at[0], w_read),
        (write_far.at[1], next_write),
        (read_far.at[1], next_read),
        (conv_far, conv),
        (taps_far, taps),
    ]
    for copy in start_all(pairs, sems):
        copy.wait()
    inv = scale_tokens(lambda j: hid[:, 128 * j : 128 * j + 128], gain.at[:1], scaled)
    inv_out[...] = jnp.broadcast_to(inv, (B, 128))
    inv_row = as_row(inv)
    mixed, later, last_taps = [], [], []
    for kind, weight in ((0, w_write), (1, w_read)):
        fresh = dot_nt(weight[...], scaled[...]) * inv_row
        old, newer = conv[0, 0, kind], conv[0, 1, kind]
        tap = [[as_col(taps[layer, k, kind : kind + 1, :]) for k in range(3)] for layer in range(2)]
        mixed.append(silu(old * tap[0][0] + newer * tap[0][1] + fresh * tap[0][2]))
        later.append(conv[1, 0, kind] * tap[1][0] + conv[1, 1, kind] * tap[1][1])
        last_taps.append(tap[1][2])
        conv_out[0, kind] = newer
        conv_out[1, kind] = fresh
    mixed_hi, mixed_lo = zip(*(hi_lo(v) for v in mixed))
    taps_hi, taps_lo = zip(*(hi_lo(v) for v in last_taps))
    first = jnp.concatenate([*mixed_hi, *later], axis=1)
    lane = lax.broadcasted_iota(jnp.int32, (4, B), 1)
    tail = jnp.zeros((4, B), F32)
    for at, col in enumerate((taps_hi[0], taps_lo[0], taps_hi[1], taps_lo[1])):
        tail = jnp.where(lane == at, col, tail)
    second = jnp.concatenate([*mixed_lo, tail, jnp.zeros((4, B), F32)], axis=1)
    row = lax.broadcasted_iota(jnp.int32, (4, 128), 0)
    for col in range(4):
        one = slice(col, col + 1)
        base = jnp.where(row == 2, first[one], second[one])
        for place in range(32):
            cols = slice(128 * place, 128 * place + 128)
            write = next_write[:, cols].astype(F32)[one]
            read = next_read[:, cols].astype(F32)[one]
            tile = jnp.where(row == 0, write, jnp.where(row == 1, read, base)).astype(BF16)
            at = 128 * (place % 2) + 16 * col + place // 2
            msg[at] = tile
            msg[at + 64] = tile


def make_keys(tokens, far):
    scratch = [((2, D), F32)] + [KEY_WEIGHTS] * 4 + [((2, 2, 2, 4, B), F32), ((2, 3, 2, 4), F32)]
    return call(
        keys_kernel,
        "keys",
        [],
        [tokens, *far],
        [
            shaped((256, 4, 128), BF16),
            pltpu.VMEM((2, 2, 4, B), F32),
            pltpu.VMEM((B, D), BF16),
            pltpu.VMEM((B, 128), F32),
            pltpu.VMEM((B, D), BF16),
        ],
        [pltpu.VMEM(*p) for p in scratch] + [pltpu.SemaphoreType.DMA((8,))],
    )


def of_head(table):
    head = lax.axis_index(("z", "y", "x"))
    mine = lax.broadcasted_iota(jnp.int32, (1, 128), 1) == head
    return jnp.sum(jnp.where(mine, table, 0.0), axis=1, keepdims=True)


def gated_values(layer, gate, fresh, raw, tables, conv, taps):
    bias, rate, skip = (t[layer : layer + 1, :] for t in tables)
    old, newer = conv[:, 0, :], conv[:, 1, :]
    tap = [taps[k, layer : layer + 1, :] for k in range(3)]
    values = silu(old * tap[0] + newer * tap[1] + fresh * tap[2])
    raw = raw + of_head(bias)
    delta = jnp.maximum(raw, 0.0) + jnp.log1p(jnp.exp(-jnp.abs(raw)))
    decay = jnp.exp(-delta * of_head(rate))
    return (delta * values).T, of_head(skip) * values, silu(gate), decay


STATE = ((B, CH, N), F32)
OUT = ((CH, D), BF16)
ROWS = 80
NOW_FAR = (((CH, D), BF16), ((CH, D), BF16), ((D, 128), BF16))
NEXT_FAR = (((D, 128), BF16), KEY_WEIGHTS, KEY_WEIGHTS)
KEPT = (
    STATE,
    OUT,
    ((2, CH), F32),
    STATE,
    OUT,
    ((2, D), F32),
    ((2, 128), F32),
    ((2, 128), F32),
    ((2, 128), F32),
    ((2, B, 2, CH), F32),
    ((3, 2, CH), F32),
    ((2, 2, 2, 4, B), F32),
)


def values_kernel(scaled, inv, *refs):
    far, refs = refs[:15], refs[15:]
    packed, decay_out, conv_out, stack, *kept = refs[: 4 + len(KEPT)]
    w_gate, w_value, w_step, next_step, next_write, next_read, sems, late_sems = refs[4 + len(KEPT) :]
    gate_far, value_far, step_far, write_far, read_far, state_far, out_far, *tables_far = far
    tables_group, tables_rest = tables_far[0], tables_far[1:]
    late_sources = [
        state_far.at[0], out_far.at[0], tables_group, state_far.at[1], out_far.at[1], *tables_rest
    ]
    late = list(zip(late_sources, kept))
    small = [(src, dst) for src, dst in late[6:11]]
    now = [(gate_far.at[0], w_gate), (value_far.at[0], w_value), (step_far.at[0], w_step)] + small
    copies = start_all(now, sems)
    late = late[:6] + late[11:]
    late += [
        (gate_far.at[1], stack.at[:CH]),
        (value_far.at[1], stack.at[CH : 2 * CH]),
        (step_far.at[1], next_step),
        (write_far.at[1], next_write),
        (read_far.at[1], next_read),
    ]
    late = start_all(late, late_sems)
    for copy in copies:
        copy.wait()
    hidden = scaled[...]
    inv_col = inv[:, :CH]
    gate = dot_nt(hidden, w_gate[...]) * inv_col
    fresh = dot_nt(hidden, w_value[...]) * inv_col
    raw = of_head(jnp.dot(hidden, w_step[...], preferred_element_type=F32) * inv[...])
    tables, conv, taps = kept[6:9], kept[9], kept[10]
    push, direct, gate, decay = gated_values(0, gate, fresh, raw, tables, conv.at[0], taps)
    packed[0] = push
    packed[1] = direct
    packed[2] = gate
    decay_out[...] = jnp.broadcast_to(decay, (B, N))
    conv_out[:, 0, :] = conv[0, :, 1, :]
    conv_out[:, 1, :] = fresh
    for copy in late:
        copy.wait()
    head = lax.axis_index(("z", "y", "x"))
    hot = (lax.broadcasted_iota(jnp.int32, (8, 128), 1) == head).astype(F32).astype(BF16)
    stack[2 * CH : 2 * CH + 8] = dot_nt(hot, next_step[...]).astype(BF16)
    both = jnp.concatenate([next_write[...].astype(F32), next_read[...].astype(F32)], axis=0)
    stack[2 * CH + 8 :] = both.astype(BF16)


def make_values(scaled, inv, far):
    outs = [pltpu.VMEM((3, B, CH), F32), pltpu.VMEM((B, N), F32)]
    outs += [pltpu.VMEM((B, 2, CH), F32), pltpu.VMEM((ROWS, D), BF16)]
    outs += [pltpu.VMEM(*p) for p in KEPT]
    scratch = [pltpu.VMEM(*p) for p in NOW_FAR + NEXT_FAR]
    scratch += [pltpu.SemaphoreType.DMA((8,)), pltpu.SemaphoreType.DMA((12,))]
    return call(values_kernel, "values", [scaled, inv], far, outs, scratch)


def advance(layer, push, direct, gate, writes, reads, state, w_out, gain, sent, states, scratch):
    fresh, decay_rows, read_rows, sems = scratch
    read_rows[...] = reads
    high, low = hi_lo(push)
    left = jnp.concatenate([high, high, low], axis=1)
    high, low = hi_lo(writes)
    right = jnp.concatenate([high, low, high], axis=0).astype(BF16)
    of = lax.broadcasted_iota(jnp.int32, left.shape, 1) % B
    left = jnp.concatenate([jnp.where(of == b, left, 0.0).astype(BF16) for b in range(B)], axis=0)
    pushed = jnp.dot(left, right, preferred_element_type=F32)
    lane = lax.broadcasted_iota(jnp.int32, (CH, B), 1)
    found = jnp.zeros((CH, B), F32)
    copies = []
    for b in range(B):
        new = decay_rows[b : b + 1, :] * state[b] + pushed[CH * b : CH * (b + 1)]
        fresh[b] = new
        total = jnp.sum(new * read_rows[b : b + 1, :], axis=1, keepdims=True)
        found = jnp.where(lane == b, total, found)
        if b % 8 == 7:
            part = pl.ds(b - 7, 8)
            copies.append(pltpu.make_async_copy(fresh.at[part], states.at[layer, part], sems.at[b // 8]))
            copies[-1].start()
    gated = (found.T + direct) * gate
    total = as_row(jnp.sum(gated * gated, axis=1, keepdims=True))
    high, low = hi_lo(total)
    tail = jnp.where(lax.broadcasted_iota(jnp.int32, (2, B), 0) == 0, high, low)
    tail = jnp.concatenate([tail, jnp.zeros((2, 128 - B), F32)], axis=1).astype(BF16)
    out = jnp.dot((gated * gain).astype(BF16), w_out[...], preferred_element_type=F32)
    for j in range(D // 128):
        sent[LINES * j : LINES * j + B] = out[:, 128 * j : 128 * j + 128].astype(BF16)
        sent[LINES * j + B : LINES * (j + 1)] = tail
    for copy in copies:
        copy.wait()


STATES = ((2, B, CH, N), F32)
ADVANCE = (STATE, ((B, N), F32), ((B, N), F32))


def advance_scratch():
    return [pltpu.VMEM(*p) for p in ADVANCE] + [pltpu.SemaphoreType.DMA((4,))]


PLANE_SUMS = ((32 * LINES, 128), BF16)


def first_mix_kernel(keys, packed, decay, state, w_out, gain, states, sent, weights, later, last_taps, lines, *scratch):
    lines[...] = keys[lax.axis_index("z") // 4].astype(F32)
    weights[0] = lines[pl.ds(0, N, stride=4), :].astype(BF16)
    weights[1] = lines[pl.ds(1, N, stride=4), :].astype(BF16)
    first = lines[pl.ds(2, N, stride=4), :].T
    second = lines[pl.ds(3, N, stride=4), :].T
    later[0] = first[2 * B : 3 * B]
    later[1] = first[3 * B :]
    last_taps[...] = second[2 * B : 2 * B + 8]
    writes = first[:B] + second[:B]
    reads = first[B : 2 * B] + second[B : 2 * B]
    scratch[1][...] = decay[...]
    advance(
        0, packed[0], packed[1], packed[2], writes, reads, state, w_out, gain[:1, :], sent, states, scratch
    )


def first_mix(keys, packed, decay, kept):
    return call(
        first_mix_kernel,
        "mix0",
        [keys, packed, decay, *kept],
        [],
        [
            pltpu.HBM(*STATES),
            pltpu.VMEM(*PLANE_SUMS),
            pltpu.VMEM((2, N, 128), BF16),
            pltpu.VMEM((2, B, N), F32),
            pltpu.VMEM((8, N), F32),
        ],
        [pltpu.VMEM((4 * N, 128), F32)] + advance_scratch(),
    )


def next_mix_kernel(own, other, stack, later, last_taps, state, w_out, gain, norm_gain, *refs):
    tables, conv, taps, key_conv, key_before, value_before = refs[:3], refs[3], refs[4], refs[5], refs[6], refs[7]
    states, sent, key_out, value_out, hid, scaled, *scratch = refs[9:]
    core = lax.axis_index("c")
    sums = [jnp.zeros((B, N), F32), jnp.zeros((B, N), F32)]
    for at in range(16):
        for whose, side in ((own, core), (other, 1 - core)):
            hid[2 * at + side] = whose[at, :B]
            for kind in range(2):
                sums[kind] += whose[at, B * (kind + 1) : B * (kind + 2)].astype(F32)
    inv = scale_tokens(lambda j: hid[j], norm_gain.at[1:], scaled)
    found = dot_nt(scaled[...], stack[...]) * inv
    keys = [silu(later[k] + sums[k] * inv * (last_taps[2 * k : 2 * k + 1] + last_taps[2 * k + 1 : 2 * k + 2])) for k in range(2)]
    fresh_values = found[:, CH : 2 * CH]
    push, direct, gate, decay = gated_values(
        1, found[:, :CH], fresh_values, found[:, 2 * CH : 2 * CH + 1], tables, conv.at[1], taps
    )
    scratch[1][...] = jnp.broadcast_to(decay, (B, N))
    advance(1, push, direct, gate, keys[0], keys[1], state, w_out, gain[1:, :], sent, states, scratch)
    value_out[0] = value_before[...]
    value_out[1, :, 0, :] = conv[1, :, 1, :]
    value_out[1, :, 1, :] = fresh_values
    turned = found.T
    key_out[0] = key_before[...]
    for kind in range(2):
        key_out[1, 0, kind] = key_conv[1, 1, kind]
        key_out[1, 1, kind] = turned[2 * CH + 8 + 4 * kind : 2 * CH + 12 + 4 * kind]


def next_mix(own, other, stack, later, last_taps, kept, key_before, value_before, states):
    return call(
        next_mix_kernel,
        "mix1",
        [own, other, stack, later, last_taps, *kept, key_before, value_before],
        [states],
        [
            pltpu.HBM(*STATES),
            pltpu.VMEM(*PLANE_SUMS),
            shaped((2, 2, 2, 4, B), F32),
            shaped((2, B, 2, CH), F32),
        ],
        [pltpu.VMEM((32, B, 128), BF16), pltpu.VMEM((B, D), BF16)] + advance_scratch(),
        {17: 0},
    )


def scale_kernel(got, sent):
    total = got[:B].astype(F32)
    squares = got[B:LINES].astype(F32)
    for j in range(1, 32):
        total += got[LINES * j : LINES * j + B].astype(F32)
        squares += got[LINES * j + B : LINES * (j + 1)].astype(F32)
    squares = squares[:1, :B] + squares[1:, :B]
    factor = as_col(lax.rsqrt(squares / GW + EPS))
    chunk = (total * factor).astype(BF16)
    for plane in range(8):
        sent[plane] = chunk


def make_scale(got):
    return call(scale_kernel, "scale", [got], [], [pltpu.VMEM((8, B, 128), BF16)])[0]


def first_add_kernel(got, hid, norm_gain, weights, sent):
    total = got[0].astype(F32)
    for plane in range(1, 8):
        total += got[plane].astype(F32)
    cols = pl.ds(pl.multiple_of(128 * lax.axis_index(PLANE), 128), 128)
    chunk = (hid[:, cols].astype(F32) + total).astype(BF16)
    scaled = (chunk.astype(F32) * norm_gain[1:, cols]).astype(BF16)
    shares = [dot_nt(scaled, weights[kind]).astype(BF16) for kind in range(2)]
    for j in range(16):
        sent[j, :B] = chunk
        sent[j, B : 2 * B] = shares[0]
        sent[j, 2 * B :] = shares[1]


def next_add_kernel(got, hid, sent):
    total = got[0].astype(F32)
    for plane in range(1, 8):
        total += got[plane].astype(F32)
    chunk = (hid[lax.axis_index(("y", "x")), :B].astype(F32) + total).astype(BF16)
    for j in range(32):
        sent[j] = chunk


def exchange(value, axes):
    return lax.all_to_all(value, axes, split_axis=0, concat_axis=0, tiled=True)


def per_device(
    tokens,
    norm_gain,
    w_gate,
    w_value,
    w_write,
    w_read,
    w_step,
    step_bias,
    decay_rate,
    skip_gain,
    conv_value_weight,
    conv_key_weight,
    group_gain,
    w_out,
    ssm_state,
    conv_value,
    conv_key,
):
    w_gate, w_value, w_write, w_read = (jnp.swapaxes(w, 1, 2) for w in (w_gate, w_value, w_write, w_read))
    conv_key = jnp.transpose(conv_key, (0, 2, 3, 4, 1))
    value_taps = jnp.swapaxes(conv_value_weight, 0, 1)
    far = [w_gate, w_value, w_step, w_write, w_read, ssm_state, w_out, group_gain, norm_gain]
    far += [step_bias, decay_rate, skip_gain, conv_value, value_taps, conv_key]
    msg, key_out, scaled, inv, hid = make_keys(tokens, [norm_gain, w_write, w_read, conv_key, conv_key_weight])
    keys = exchange(msg, ("c", "z", "y", "x")).reshape(2, 4 * N, 128)
    packed, decay, value_out, stack, *kept = make_values(scaled, inv, far)
    state, out, gain, next_state, next_out, *rest = kept
    states, sent, weights, later, last_taps = first_mix(keys, packed, decay, [state, out, gain])
    sent = make_scale(exchange(sent.reshape(32, LINES // 2, 2, 128), PLANE).reshape(sent.shape))
    (sent,) = call(
        first_add_kernel,
        "add0",
        [exchange(sent, ("z",)), hid, rest[0], weights],
        [],
        [pltpu.VMEM((16, 3 * B, 128), BF16)],
    )
    own = exchange(sent, ("y", "x"))
    other = lax.ppermute(own, "c", [(0, 1), (1, 0)])
    states, sent, key_out, value_out = next_mix(
        own, other, stack, later, last_taps, [next_state, next_out, gain, *rest], key_out, value_out, states
    )
    sent = make_scale(exchange(sent.reshape(32, LINES // 2, 2, 128), PLANE).reshape(sent.shape))
    (sent,) = call(next_add_kernel, "add1", [exchange(sent, ("z",)), own], [], [pltpu.VMEM((32, B, 128), BF16)])
    hid = exchange(sent, PLANE)
    tokens_out = jnp.transpose(hid, (1, 0, 2)).reshape(B, D)
    return (tokens_out, states, value_out, jnp.transpose(key_out, (0, 4, 1, 2, 3)))


def solution(mesh):
    torus = Mesh(mesh.devices.reshape(8, 4, 4, 2), TP)
    in_specs = (
        P(),
        P(),
        P(None, None, TP),
        P(None, None, TP),
        P(None, None, TP),
        P(None, None, TP),
        P(),
        P(),
        P(),
        P(),
        P(None, None, TP),
        P(None, None, None, TP),
        P(None, TP),
        P(None, TP, None),
        P(None, None, TP, None),
        P(None, None, None, TP),
        P(None, None, None, None, TP),
    )
    out_specs = (
        P(),
        P(None, None, TP, None),
        P(None, None, None, TP),
        P(None, None, None, None, TP),
    )
    return jax.shard_map(
        per_device, mesh=torus, in_specs=in_specs, out_specs=out_specs, check_vma=False
    )
```

```python
import functools

import jax
import jax.numpy as jnp
from jax import lax
from jax.experimental import pallas as pl
from jax.experimental.pallas import tpu as pltpu
from jax.sharding import Mesh
from jax.sharding import PartitionSpec as P

D = 4096
B = 32
CH = 32
N = 128
GW = 1024
LINES = B + 2
EPS = 1e-06
TP = ("z", "y", "x", "c")
PLANE = ("y", "x", "c")
F32 = jnp.float32
BF16 = jnp.bfloat16


LIMIT = pltpu.CompilerParams(vmem_limit_bytes=8 * 1024 * 1024)


def vmem():
    return pl.BlockSpec(memory_space=pltpu.VMEM)


def anywhere():
    return pl.BlockSpec(memory_space=pl.ANY)


def shaped(shape, dtype):
    return jax.ShapeDtypeStruct(shape, dtype)


def start_all(pairs, sems):
    copies = [pltpu.make_async_copy(src, dst, sems.at[at]) for at, (src, dst) in enumerate(pairs)]
    for copy in copies:
        copy.start()
    return copies


def call(body, name, near, far, outs, scratch=(), aliases=None):
    near = [pltpu.with_memory_space_constraint(v, pltpu.VMEM) for v in near]
    far = [pltpu.with_memory_space_constraint(v, pltpu.HBM) for v in far]
    far_out = (pltpu.HBM((1,), F32).memory_space,)
    specs = [anywhere() if getattr(o, "memory_space", None) in far_out else vmem() for o in outs]
    return pl.pallas_call(
        body,
        in_specs=[vmem()] * len(near) + [anywhere()] * len(far),
        out_specs=specs,
        out_shape=list(outs),
        scratch_shapes=list(scratch),
        input_output_aliases=aliases or {},
        compiler_params=LIMIT,
        name=name,
    )(*near, *far)


def silu(v):
    return v / (1.0 + jnp.exp(-v))


def as_col(row):
    n = row.shape[1]
    at = lax.broadcasted_iota(jnp.int32, (n, n), 0)
    of = lax.broadcasted_iota(jnp.int32, (n, n), 1)
    return jnp.sum(jnp.where(at == of, row, 0.0), axis=1, keepdims=True)


def as_row(col):
    n = col.shape[0]
    at = lax.broadcasted_iota(jnp.int32, (n, n), 0)
    of = lax.broadcasted_iota(jnp.int32, (n, n), 1)
    return jnp.sum(jnp.where(at == of, col, 0.0), axis=0, keepdims=True)


def dot_nt(a, b):
    return lax.dot_general(a, b, (((1,), (1,)), ((), ())), preferred_element_type=F32)


def hi_lo(value):
    high = value.astype(BF16).astype(F32)
    return high, value - high


def scale_tokens(part_of, gain, scaled):
    squares = jnp.zeros((B, 128), F32)
    for j in range(D // 128):
        cols = slice(128 * j, 128 * j + 128)
        part = part_of(j).astype(F32)
        squares += part * part
        scaled[:, cols] = (part * gain[:, cols]).astype(BF16)
    return lax.rsqrt(jnp.sum(squares, axis=1, keepdims=True) / D + EPS)


KEY_WEIGHTS = ((4, D), BF16)
KEY_PARAMS = (((2, 4, D), BF16), ((2, 4, D), BF16), ((2, 2, 2, 4, B), F32), ((2, 3, 2, 4), F32))


def start_kernel(tokens, gain_far, *refs):
    far, (scaled, inv_out, hid), near, (gain, sems, late_sems) = refs[:4], refs[4:7], refs[7:11], refs[11:]
    copies = start_all([(tokens, hid), (gain_far, gain)], sems)
    late = start_all(list(zip(far, near)), late_sems)
    for copy in copies:
        copy.wait()
    inv = scale_tokens(lambda j: hid[:, 128 * j : 128 * j + 128], gain.at[:1], scaled)
    inv_out[...] = jnp.broadcast_to(inv, (B, 128))
    for copy in late:
        copy.wait()


def make_start(tokens, gain, far):
    outs = [((B, D), BF16), ((B, 128), F32), ((B, D), BF16), *KEY_PARAMS]
    return call(
        start_kernel,
        "start",
        [],
        [tokens, gain, *far],
        [pltpu.VMEM(*p) for p in outs],
        [pltpu.VMEM((2, D), F32), pltpu.SemaphoreType.DMA((2,)), pltpu.SemaphoreType.DMA((4,))],
    )


def keys_kernel(scaled, inv, *refs):
    sides, (msg, conv_out) = (refs[:4], refs[4:8]), refs[8:]
    core = lax.axis_index("c")
    rows = [weight[0].astype(F32) for side in sides for weight in side[:2]]
    found = dot_nt(jnp.concatenate(rows, axis=0).astype(BF16), scaled[...]) * as_row(inv[:, :1])
    lane = lax.broadcasted_iota(jnp.int32, (4, B), 1)
    row = lax.broadcasted_iota(jnp.int32, (4, 128), 0)
    for of, (w_write, w_read, conv, taps) in enumerate(sides):
        mixed, later, last_taps = [], [], []
        for kind in range(2):
            at = 8 * of + 4 * kind
            fresh = found[at : at + 4]
            old, newer = conv[0, 0, kind], conv[0, 1, kind]
            tap = [[as_col(taps[layer, k, kind : kind + 1, :]) for k in range(3)] for layer in range(2)]
            mixed.append(silu(old * tap[0][0] + newer * tap[0][1] + fresh * tap[0][2]))
            later.append(conv[1, 0, kind] * tap[1][0] + conv[1, 1, kind] * tap[1][1])
            last_taps.append(tap[1][2])
            if not of:
                conv_out[0, kind] = newer
                conv_out[1, kind] = fresh
        mixed_hi, mixed_lo = zip(*(hi_lo(v) for v in mixed))
        taps_hi, taps_lo = zip(*(hi_lo(v) for v in last_taps))
        first = jnp.concatenate([*mixed_hi, *later], axis=1)
        tail = jnp.zeros((4, B), F32)
        for at, col in enumerate((taps_hi[0], taps_lo[0], taps_hi[1], taps_lo[1])):
            tail = jnp.where(lane == at, col, tail)
        second = jnp.concatenate([*mixed_lo, tail, jnp.zeros((4, B), F32)], axis=1)
        base = [jnp.where(row == 2, first[col : col + 1], second[col : col + 1]) for col in range(4)]
        start = 64 * (1 - core if of else core)
        for place in range(16):
            cols = pl.ds(pl.multiple_of(128 * (2 * place + core), 128), 128)
            writes = w_write[1, :, cols].astype(F32)
            reads = w_read[1, :, cols].astype(F32)
            for col in range(4):
                one = slice(col, col + 1)
                tile = jnp.where(row == 0, writes[one], jnp.where(row == 1, reads[one], base[col]))
                msg[start + 16 * col + place] = tile.astype(BF16)


def make_keys(scaled, inv, own, other):
    return call(
        keys_kernel,
        "keys",
        [scaled, inv, *own, *other],
        [],
        [shaped((128, 4, 128), BF16), pltpu.VMEM((2, 2, 4, B), F32)],
    )


def of_head(table):
    head = lax.axis_index(("z", "y", "x"))
    mine = lax.broadcasted_iota(jnp.int32, (1, 128), 1) == head
    return jnp.sum(jnp.where(mine, table, 0.0), axis=1, keepdims=True)


def gated_values(layer, gate, fresh, raw, tables, conv, taps):
    bias, rate, skip = (t[layer : layer + 1, :] for t in tables)
    old, newer = conv[:, 0, :], conv[:, 1, :]
    tap = [taps[k, layer : layer + 1, :] for k in range(3)]
    values = silu(old * tap[0] + newer * tap[1] + fresh * tap[2])
    raw = raw + of_head(bias)
    delta = jnp.maximum(raw, 0.0) + jnp.log1p(jnp.exp(-jnp.abs(raw)))
    decay = jnp.exp(-delta * of_head(rate))
    return (delta * values).T, of_head(skip) * values, silu(gate), decay


STATE = ((B, CH, N), F32)
OUT = ((CH, D), BF16)
ROWS = 80
NOW_FAR = (((CH, D), BF16), ((CH, D), BF16), ((D, 128), BF16))
NEXT_FAR = (((D, 128), BF16), KEY_WEIGHTS, KEY_WEIGHTS)
KEPT = (
    STATE,
    OUT,
    ((2, CH), F32),
    STATE,
    OUT,
    ((2, D), F32),
    ((2, 128), F32),
    ((2, 128), F32),
    ((2, 128), F32),
    ((2, B, 2, CH), F32),
    ((3, 2, CH), F32),
    ((2, 2, 2, 4, B), F32),
)


def values_kernel(scaled, inv, *refs):
    far, refs = refs[:15], refs[15:]
    packed, decay_out, conv_out, stack, *kept = refs[: 4 + len(KEPT)]
    w_gate, w_value, w_step, next_step, next_write, next_read, sems, late_sems = refs[4 + len(KEPT) :]
    gate_far, value_far, step_far, write_far, read_far, state_far, out_far, *tables_far = far
    tables_group, tables_rest = tables_far[0], tables_far[1:]
    late_sources = [
        state_far.at[0], out_far.at[0], tables_group, state_far.at[1], out_far.at[1], *tables_rest
    ]
    late = list(zip(late_sources, kept))
    small = [(src, dst) for src, dst in late[6:11]]
    now = [(gate_far.at[0], w_gate), (value_far.at[0], w_value), (step_far.at[0], w_step)] + small
    copies = start_all(now, sems)
    late = late[:6] + late[11:]
    late += [
        (gate_far.at[1], stack.at[:CH]),
        (value_far.at[1], stack.at[CH : 2 * CH]),
        (step_far.at[1], next_step),
        (write_far.at[1], next_write),
        (read_far.at[1], next_read),
    ]
    late = start_all(late, late_sems)
    for copy in copies:
        copy.wait()
    hidden = scaled[...]
    inv_col = inv[:, :CH]
    gate = dot_nt(hidden, w_gate[...]) * inv_col
    fresh = dot_nt(hidden, w_value[...]) * inv_col
    raw = of_head(jnp.dot(hidden, w_step[...], preferred_element_type=F32) * inv[...])
    tables, conv, taps = kept[6:9], kept[9], kept[10]
    push, direct, gate, decay = gated_values(0, gate, fresh, raw, tables, conv.at[0], taps)
    packed[0] = push
    packed[1] = direct
    packed[2] = gate
    decay_out[...] = jnp.broadcast_to(decay, (B, N))
    conv_out[:, 0, :] = conv[0, :, 1, :]
    conv_out[:, 1, :] = fresh
    for copy in late:
        copy.wait()
    head = lax.axis_index(("z", "y", "x"))
    hot = (lax.broadcasted_iota(jnp.int32, (8, 128), 1) == head).astype(F32).astype(BF16)
    stack[2 * CH : 2 * CH + 8] = dot_nt(hot, next_step[...]).astype(BF16)
    both = jnp.concatenate([next_write[...].astype(F32), next_read[...].astype(F32)], axis=0)
    stack[2 * CH + 8 :] = both.astype(BF16)


def make_values(scaled, inv, far):
    outs = [pltpu.VMEM((3, B, CH), F32), pltpu.VMEM((B, N), F32)]
    outs += [pltpu.VMEM((B, 2, CH), F32), pltpu.VMEM((ROWS, D), BF16)]
    outs += [pltpu.VMEM(*p) for p in KEPT]
    scratch = [pltpu.VMEM(*p) for p in NOW_FAR + NEXT_FAR]
    scratch += [pltpu.SemaphoreType.DMA((8,)), pltpu.SemaphoreType.DMA((12,))]
    return call(values_kernel, "values", [scaled, inv], far, outs, scratch)


def advance(layer, push, direct, gate, writes, reads, state, w_out, gain, sent, states, scratch):
    fresh, decay_rows, read_rows, sems = scratch
    read_rows[...] = reads
    high, low = hi_lo(push)
    left = jnp.concatenate([high, high, low], axis=1)
    high, low = hi_lo(writes)
    right = jnp.concatenate([high, low, high], axis=0).astype(BF16)
    of = lax.broadcasted_iota(jnp.int32, left.shape, 1) % B
    left = jnp.concatenate([jnp.where(of == b, left, 0.0).astype(BF16) for b in range(B)], axis=0)
    pushed = jnp.dot(left, right, preferred_element_type=F32)
    lane = lax.broadcasted_iota(jnp.int32, (CH, B), 1)
    found = jnp.zeros((CH, B), F32)
    copies = []
    for b in range(B):
        new = decay_rows[b : b + 1, :] * state[b] + pushed[CH * b : CH * (b + 1)]
        fresh[b] = new
        total = jnp.sum(new * read_rows[b : b + 1, :], axis=1, keepdims=True)
        found = jnp.where(lane == b, total, found)
        if b % 8 == 7:
            part = pl.ds(b - 7, 8)
            copies.append(pltpu.make_async_copy(fresh.at[part], states.at[layer, part], sems.at[b // 8]))
            copies[-1].start()
    gated = (found.T + direct) * gate
    total = as_row(jnp.sum(gated * gated, axis=1, keepdims=True))
    high, low = hi_lo(total)
    tail = jnp.where(lax.broadcasted_iota(jnp.int32, (2, B), 0) == 0, high, low)
    tail = jnp.concatenate([tail, jnp.zeros((2, 128 - B), F32)], axis=1).astype(BF16)
    out = jnp.dot((gated * gain).astype(BF16), w_out[...], preferred_element_type=F32)
    for j in range(D // 128):
        sent[LINES * j : LINES * j + B] = out[:, 128 * j : 128 * j + 128].astype(BF16)
        sent[LINES * j + B : LINES * (j + 1)] = tail
    for copy in copies:
        copy.wait()


STATES = ((2, B, CH, N), F32)
ADVANCE = (STATE, ((B, N), F32), ((B, N), F32))


def advance_scratch():
    return [pltpu.VMEM(*p) for p in ADVANCE] + [pltpu.SemaphoreType.DMA((4,))]


PLANE_SUMS = ((32 * LINES, 128), BF16)


def first_mix_kernel(keys, packed, decay, state, w_out, gain, states, sent, weights, later, last_taps, lines, *scratch):
    lines[...] = keys[...].astype(F32)
    weights[0] = lines[pl.ds(0, N, stride=4), :].astype(BF16)
    weights[1] = lines[pl.ds(1, N, stride=4), :].astype(BF16)
    first = lines[pl.ds(2, N, stride=4), :].T
    second = lines[pl.ds(3, N, stride=4), :].T
    later[0] = first[2 * B : 3 * B]
    later[1] = first[3 * B :]
    last_taps[...] = second[2 * B : 2 * B + 8]
    writes = first[:B] + second[:B]
    reads = first[B : 2 * B] + second[B : 2 * B]
    scratch[1][...] = decay[...]
    advance(
        0, packed[0], packed[1], packed[2], writes, reads, state, w_out, gain[:1, :], sent, states, scratch
    )


def first_mix(keys, packed, decay, kept):
    return call(
        first_mix_kernel,
        "mix0",
        [keys, packed, decay, *kept],
        [],
        [
            pltpu.HBM(*STATES),
            pltpu.VMEM(*PLANE_SUMS),
            pltpu.VMEM((2, N, 128), BF16),
            pltpu.VMEM((2, B, N), F32),
            pltpu.VMEM((8, N), F32),
        ],
        [pltpu.VMEM((4 * N, 128), F32)] + advance_scratch(),
    )


def next_mix_kernel(own, other, stack, later, last_taps, state, w_out, gain, norm_gain, *refs):
    tables, conv, taps, key_conv, key_before, value_before = refs[:3], refs[3], refs[4], refs[5], refs[6], refs[7]
    states, sent, key_out, value_out, hid, scaled, *scratch = refs[9:]
    core = lax.axis_index("c")
    sums = [jnp.zeros((B, N), F32), jnp.zeros((B, N), F32)]
    for at in range(16):
        for whose, side in ((own, core), (other, 1 - core)):
            hid[2 * at + side] = whose[at, :B]
            for kind in range(2):
                sums[kind] += whose[at, B * (kind + 1) : B * (kind + 2)].astype(F32)
    inv = scale_tokens(lambda j: hid[j], norm_gain.at[1:], scaled)
    found = dot_nt(scaled[...], stack[...]) * inv
    keys = [silu(later[k] + sums[k] * inv * (last_taps[2 * k : 2 * k + 1] + last_taps[2 * k + 1 : 2 * k + 2])) for k in range(2)]
    fresh_values = found[:, CH : 2 * CH]
    push, direct, gate, decay = gated_values(
        1, found[:, :CH], fresh_values, found[:, 2 * CH : 2 * CH + 1], tables, conv.at[1], taps
    )
    scratch[1][...] = jnp.broadcast_to(decay, (B, N))
    advance(1, push, direct, gate, keys[0], keys[1], state, w_out, gain[1:, :], sent, states, scratch)
    value_out[0] = value_before[...]
    value_out[1, :, 0, :] = conv[1, :, 1, :]
    value_out[1, :, 1, :] = fresh_values
    turned = found.T
    key_out[0] = key_before[...]
    for kind in range(2):
        key_out[1, 0, kind] = key_conv[1, 1, kind]
        key_out[1, 1, kind] = turned[2 * CH + 8 + 4 * kind : 2 * CH + 12 + 4 * kind]


def next_mix(own, other, stack, later, last_taps, kept, key_before, value_before, states):
    return call(
        next_mix_kernel,
        "mix1",
        [own, other, stack, later, last_taps, *kept, key_before, value_before],
        [states],
        [
            pltpu.HBM(*STATES),
            pltpu.VMEM(*PLANE_SUMS),
            shaped((2, 2, 2, 4, B), F32),
            shaped((2, B, 2, CH), F32),
        ],
        [pltpu.VMEM((32, B, 128), BF16), pltpu.VMEM((B, D), BF16)] + advance_scratch(),
        {17: 0},
    )


def scale_kernel(got, sent):
    total = got[:B].astype(F32)
    squares = got[B:LINES].astype(F32)
    for j in range(1, 32):
        total += got[LINES * j : LINES * j + B].astype(F32)
        squares += got[LINES * j + B : LINES * (j + 1)].astype(F32)
    squares = squares[:1, :B] + squares[1:, :B]
    factor = as_col(lax.rsqrt(squares / GW + EPS))
    chunk = (total * factor).astype(BF16)
    for plane in range(8):
        sent[plane] = chunk


def make_scale(got):
    return call(scale_kernel, "scale", [got], [], [pltpu.VMEM((8, B, 128), BF16)])[0]


def first_add_kernel(got, hid, norm_gain, weights, sent):
    total = got[0].astype(F32)
    for plane in range(1, 8):
        total += got[plane].astype(F32)
    cols = pl.ds(pl.multiple_of(128 * lax.axis_index(PLANE), 128), 128)
    chunk = (hid[:, cols].astype(F32) + total).astype(BF16)
    scaled = (chunk.astype(F32) * norm_gain[1:, cols]).astype(BF16)
    shares = [dot_nt(scaled, weights[kind]).astype(BF16) for kind in range(2)]
    for j in range(16):
        sent[j, :B] = chunk
        sent[j, B : 2 * B] = shares[0]
        sent[j, 2 * B :] = shares[1]


def next_add_kernel(got, hid, sent):
    total = got[0].astype(F32)
    for plane in range(1, 8):
        total += got[plane].astype(F32)
    chunk = (hid[lax.axis_index(("y", "x")), :B].astype(F32) + total).astype(BF16)
    for j in range(32):
        sent[j] = chunk


def exchange(value, axes):
    return lax.all_to_all(value, axes, split_axis=0, concat_axis=0, tiled=True)


def swap(value):
    return lax.ppermute(value, "c", [(0, 1), (1, 0)])


def per_device(
    tokens,
    norm_gain,
    w_gate,
    w_value,
    w_write,
    w_read,
    w_step,
    step_bias,
    decay_rate,
    skip_gain,
    conv_value_weight,
    conv_key_weight,
    group_gain,
    w_out,
    ssm_state,
    conv_value,
    conv_key,
):
    w_gate, w_value, w_write, w_read = (jnp.swapaxes(w, 1, 2) for w in (w_gate, w_value, w_write, w_read))
    conv_key = jnp.transpose(conv_key, (0, 2, 3, 4, 1))
    value_taps = jnp.swapaxes(conv_value_weight, 0, 1)
    far = [w_gate, w_value, w_step, w_write, w_read, ssm_state, w_out, group_gain, norm_gain]
    far += [step_bias, decay_rate, skip_gain, conv_value, value_taps, conv_key]
    key_far = [w_write, w_read, conv_key, conv_key_weight]
    others = [swap(v) for v in key_far]
    scaled, inv, hid, *own = make_start(tokens, norm_gain, key_far)
    msg, key_out = make_keys(scaled, inv, own, others)
    keys = exchange(msg, ("z", "y", "x")).reshape(4 * N, 128)
    packed, decay, value_out, stack, *kept = make_values(scaled, inv, far)
    state, out, gain, next_state, next_out, *rest = kept
    states, sent, weights, later, last_taps = first_mix(keys, packed, decay, [state, out, gain])
    sent = make_scale(exchange(sent.reshape(32, LINES // 2, 2, 128), PLANE).reshape(sent.shape))
    (sent,) = call(
        first_add_kernel,
        "add0",
        [exchange(sent, ("z",)), hid, rest[0], weights],
        [],
        [pltpu.VMEM((16, 3 * B, 128), BF16)],
    )
    own = exchange(sent, ("y", "x"))
    other = swap(own)
    states, sent, key_out, value_out = next_mix(
        own, other, stack, later, last_taps, [next_state, next_out, gain, *rest], key_out, value_out, states
    )
    sent = make_scale(exchange(sent.reshape(32, LINES // 2, 2, 128), PLANE).reshape(sent.shape))
    (sent,) = call(next_add_kernel, "add1", [exchange(sent, ("z",)), own], [], [pltpu.VMEM((32, B, 128), BF16)])
    hid = exchange(sent, PLANE)
    tokens_out = jnp.transpose(hid, (1, 0, 2)).reshape(B, D)
    return (tokens_out, states, value_out, jnp.transpose(key_out, (0, 4, 1, 2, 3)))


def solution(mesh):
    torus = Mesh(mesh.devices.reshape(8, 4, 4, 2), TP)
    in_specs = (
        P(),
        P(),
        P(None, None, TP),
        P(None, None, TP),
        P(None, None, TP),
        P(None, None, TP),
        P(),
        P(),
        P(),
        P(),
        P(None, None, TP),
        P(None, None, None, TP),
        P(None, TP),
        P(None, TP, None),
        P(None, None, TP, None),
        P(None, None, None, TP),
        P(None, None, None, None, TP),
    )
    out_specs = (
        P(),
        P(None, None, TP, None),
        P(None, None, None, TP),
        P(None, None, None, None, TP),
    )
    return jax.shard_map(
        per_device, mesh=torus, in_specs=in_specs, out_specs=out_specs, check_vma=False
    )
```

```python
import functools

import jax
import jax.numpy as jnp
from jax import lax
from jax.experimental import pallas as pl
from jax.experimental.pallas import tpu as pltpu
from jax.sharding import Mesh
from jax.sharding import PartitionSpec as P

D = 4096
B = 32
CH = 32
N = 128
GW = 1024
LINES = B + 2
EPS = 1e-06
TP = ("z", "y", "x", "c")
PLANE = ("y", "x", "c")
F32 = jnp.float32
BF16 = jnp.bfloat16


LIMIT = pltpu.CompilerParams(vmem_limit_bytes=8 * 1024 * 1024)


def vmem():
    return pl.BlockSpec(memory_space=pltpu.VMEM)


def anywhere():
    return pl.BlockSpec(memory_space=pl.ANY)


def shaped(shape, dtype):
    return jax.ShapeDtypeStruct(shape, dtype)


def start_all(pairs, sems):
    copies = [pltpu.make_async_copy(src, dst, sems.at[at]) for at, (src, dst) in enumerate(pairs)]
    for copy in copies:
        copy.start()
    return copies


def call(body, name, near, far, outs, scratch=(), aliases=None):
    near = [pltpu.with_memory_space_constraint(v, pltpu.VMEM) for v in near]
    far = [pltpu.with_memory_space_constraint(v, pltpu.HBM) for v in far]
    far_out = (pltpu.HBM((1,), F32).memory_space,)
    specs = [anywhere() if getattr(o, "memory_space", None) in far_out else vmem() for o in outs]
    return pl.pallas_call(
        body,
        in_specs=[vmem()] * len(near) + [anywhere()] * len(far),
        out_specs=specs,
        out_shape=list(outs),
        scratch_shapes=list(scratch),
        input_output_aliases=aliases or {},
        compiler_params=LIMIT,
        name=name,
    )(*near, *far)


def silu(v):
    return v / (1.0 + jnp.exp(-v))


def as_col(row):
    n = row.shape[1]
    at = lax.broadcasted_iota(jnp.int32, (n, n), 0)
    of = lax.broadcasted_iota(jnp.int32, (n, n), 1)
    return jnp.sum(jnp.where(at == of, row, 0.0), axis=1, keepdims=True)


def as_row(col):
    n = col.shape[0]
    at = lax.broadcasted_iota(jnp.int32, (n, n), 0)
    of = lax.broadcasted_iota(jnp.int32, (n, n), 1)
    return jnp.sum(jnp.where(at == of, col, 0.0), axis=0, keepdims=True)


def dot_nt(a, b):
    return lax.dot_general(a, b, (((1,), (1,)), ((), ())), preferred_element_type=F32)


def hi_lo(value):
    high = value.astype(BF16).astype(F32)
    return high, value - high


def scale_tokens(part_of, gain, scaled):
    squares = jnp.zeros((B, 128), F32)
    for j in range(D // 128):
        cols = slice(128 * j, 128 * j + 128)
        part = part_of(j).astype(F32)
        squares += part * part
        scaled[:, cols] = (part * gain[:, cols]).astype(BF16)
    return lax.rsqrt(jnp.sum(squares, axis=1, keepdims=True) / D + EPS)


KEY_WEIGHTS = ((4, D), BF16)
KEY_PARAMS = (((2, 4, D), BF16), ((2, 4, D), BF16), ((2, 2, 2, 4, B), F32), ((2, 3, 2, 4), F32))


def start_kernel(tokens, gain_far, *refs):
    far, (scaled, inv_out, hid), near, (gain, sems, late_sems) = refs[:4], refs[4:7], refs[7:11], refs[11:]
    copies = start_all([(tokens, hid), (gain_far, gain)], sems)
    late = start_all(list(zip(far, near)), late_sems)
    for copy in copies:
        copy.wait()
    inv = scale_tokens(lambda j: hid[:, 128 * j : 128 * j + 128], gain.at[:1], scaled)
    inv_out[...] = jnp.broadcast_to(inv, (B, 128))
    for copy in late:
        copy.wait()


def make_start(tokens, gain, far):
    outs = [((B, D), BF16), ((B, 128), F32), ((B, D), BF16), *KEY_PARAMS]
    return call(
        start_kernel,
        "start",
        [],
        [tokens, gain, *far],
        [pltpu.VMEM(*p) for p in outs],
        [pltpu.VMEM((2, D), F32), pltpu.SemaphoreType.DMA((2,)), pltpu.SemaphoreType.DMA((4,))],
    )


def keys_kernel(scaled, inv, *refs):
    sides, (msg, conv_out) = (refs[:4], refs[4:8]), refs[8:]
    core = lax.axis_index("c")
    rows = [weight[0].astype(F32) for side in sides for weight in side[:2]]
    found = dot_nt(jnp.concatenate(rows, axis=0).astype(BF16), scaled[...]) * as_row(inv[:, :1])
    lane = lax.broadcasted_iota(jnp.int32, (4, B), 1)
    row = lax.broadcasted_iota(jnp.int32, (4, 128), 0)
    for of, (w_write, w_read, conv, taps) in enumerate(sides):
        mixed, later, last_taps = [], [], []
        for kind in range(2):
            at = 8 * of + 4 * kind
            fresh = found[at : at + 4]
            old, newer = conv[0, 0, kind], conv[0, 1, kind]
            tap = [[as_col(taps[layer, k, kind : kind + 1, :]) for k in range(3)] for layer in range(2)]
            mixed.append(silu(old * tap[0][0] + newer * tap[0][1] + fresh * tap[0][2]))
            later.append(conv[1, 0, kind] * tap[1][0] + conv[1, 1, kind] * tap[1][1])
            last_taps.append(tap[1][2])
            if not of:
                conv_out[0, kind] = newer
                conv_out[1, kind] = fresh
        mixed_hi, mixed_lo = zip(*(hi_lo(v) for v in mixed))
        taps_hi, taps_lo = zip(*(hi_lo(v) for v in last_taps))
        first = jnp.concatenate([*mixed_hi, *later], axis=1)
        tail = jnp.zeros((4, B), F32)
        for at, col in enumerate((taps_hi[0], taps_lo[0], taps_hi[1], taps_lo[1])):
            tail = jnp.where(lane == at, col, tail)
        second = jnp.concatenate([*mixed_lo, tail, jnp.zeros((4, B), F32)], axis=1)
        base = [jnp.where(row == 2, first[col : col + 1], second[col : col + 1]) for col in range(4)]
        start = 64 * (1 - core if of else core)
        for place in range(16):
            cols = pl.ds(pl.multiple_of(128 * (2 * place + core), 128), 128)
            writes = w_write[1, :, cols].astype(F32)
            reads = w_read[1, :, cols].astype(F32)
            for col in range(4):
                one = slice(col, col + 1)
                tile = jnp.where(row == 0, writes[one], jnp.where(row == 1, reads[one], base[col]))
                msg[start + 16 * col + place] = tile.astype(BF16)


def make_keys(scaled, inv, own, other):
    return call(
        keys_kernel,
        "keys",
        [scaled, inv, *own, *other],
        [],
        [shaped((128, 4, 128), BF16), pltpu.VMEM((2, 2, 4, B), F32)],
    )


def of_head(table):
    head = lax.axis_index(("z", "y", "x"))
    mine = lax.broadcasted_iota(jnp.int32, (1, 128), 1) == head
    return jnp.sum(jnp.where(mine, table, 0.0), axis=1, keepdims=True)


def steps_of(raw, rate):
    delta = jnp.maximum(raw, 0.0) + jnp.log1p(jnp.exp(-jnp.abs(raw)))
    return delta, jnp.exp(-delta * rate)


def row_of(table, layer):
    return table[layer : layer + 1, :]


STATE = ((B, CH, N), F32)
OUT = ((CH, D), BF16)
ROWS = 80
NOW_FAR = (((CH, D), BF16), ((CH, D), BF16), ((D, 128), BF16))
NEXT_FAR = (((D, 128), BF16), KEY_WEIGHTS, KEY_WEIGHTS)
KEPT = (
    STATE,
    OUT,
    ((2, CH), F32),
    STATE,
    OUT,
    ((2, D), F32),
    ((2, 128), F32),
    ((2, 128), F32),
    ((2, 128), F32),
    ((2, B, 2, CH), F32),
    ((3, 2, CH), F32),
    ((2, 2, 2, 4, B), F32),
)


def values_kernel(scaled, inv, *refs):
    far, refs = refs[:15], refs[15:]
    packed, decay_out, conv_out, halves, ready, *kept = refs[: 5 + len(KEPT)]
    w_gate, w_value, w_step, next_step, next_write, next_read, stack, sems, late_sems = refs[5 + len(KEPT) :]
    gate_far, value_far, step_far, write_far, read_far, state_far, out_far, *tables_far = far
    tables_group, tables_rest = tables_far[0], tables_far[1:]
    late_sources = [
        state_far.at[0], out_far.at[0], tables_group, state_far.at[1], out_far.at[1], *tables_rest
    ]
    late = list(zip(late_sources, kept))
    small = [(src, dst) for src, dst in late[6:11]]
    now = [(gate_far.at[0], w_gate), (value_far.at[0], w_value), (step_far.at[0], w_step)] + small
    copies = start_all(now, sems)
    late = late[:6] + late[11:]
    late += [
        (gate_far.at[1], stack.at[:CH]),
        (value_far.at[1], stack.at[CH : 2 * CH]),
        (step_far.at[1], next_step),
        (write_far.at[1], next_write),
        (read_far.at[1], next_read),
    ]
    late = start_all(late, late_sems)
    for copy in copies:
        copy.wait()
    hidden = scaled[...]
    inv_col = inv[:, :CH]
    gate = dot_nt(hidden, w_gate[...]) * inv_col
    fresh = dot_nt(hidden, w_value[...]) * inv_col
    raw = of_head(jnp.dot(hidden, w_step[...], preferred_element_type=F32) * inv[...])
    (bias, rate, skip), conv, taps = kept[6:9], kept[9], kept[10]
    tap = [[row_of(taps[k], layer) for k in range(3)] for layer in range(2)]
    values = silu(conv[0, :, 0, :] * tap[0][0] + conv[0, :, 1, :] * tap[0][1] + fresh * tap[0][2])
    delta, decay = steps_of(raw + of_head(row_of(bias, 0)), of_head(row_of(rate, 0)))
    packed[0] = (delta * values).T
    packed[1] = (of_head(row_of(skip, 0)) * values).T
    packed[2] = silu(gate).T
    decay_out[...] = jnp.broadcast_to(decay, (B, N))
    conv_out[:, 0, :] = conv[0, :, 1, :]
    conv_out[:, 1, :] = fresh
    for copy in late:
        copy.wait()
    head = lax.axis_index(("z", "y", "x"))
    hot = (lax.broadcasted_iota(jnp.int32, (8, 128), 1) == head).astype(F32).astype(BF16)
    stack[2 * CH : 2 * CH + 8] = dot_nt(hot, next_step[...]).astype(BF16)
    both = jnp.concatenate([next_write[...].astype(F32), next_read[...].astype(F32)], axis=0)
    stack[2 * CH + 8 :] = both.astype(BF16)
    for place in range(16):
        for side in range(2):
            at = 128 * (2 * place + side)
            halves[side, :, 128 * place : 128 * place + 128] = stack[:, at : at + 128]
    packed[3] = jnp.broadcast_to(as_col(row_of(kept[2], 0)), (CH, B))
    ready[0] = (conv[1, :, 0, :] * tap[1][0] + conv[1, :, 1, :] * tap[1][1]).T
    ready[1] = jnp.broadcast_to(as_col(tap[1][2]), (CH, B))
    ready[2] = jnp.broadcast_to(as_col(row_of(kept[2], 1)), (CH, B))
    for at, table in enumerate((bias, rate, skip)):
        ready[3, at : at + 1] = jnp.broadcast_to(of_head(row_of(table, 1)), (1, B))


def make_values(scaled, inv, far):
    outs = [pltpu.VMEM((4, CH, B), F32), pltpu.VMEM((B, N), F32)]
    outs += [pltpu.VMEM((B, 2, CH), F32), pltpu.VMEM((2, ROWS, D // 2), BF16), pltpu.VMEM((4, CH, B), F32)]
    outs += [pltpu.VMEM(*p) for p in KEPT]
    scratch = [pltpu.VMEM(*p) for p in (*NOW_FAR, *NEXT_FAR, ((ROWS, D), BF16))]
    scratch += [pltpu.SemaphoreType.DMA((8,)), pltpu.SemaphoreType.DMA((12,))]
    return call(values_kernel, "values", [scaled, inv], far, outs, scratch)


def advance(layer, push, direct, gate, writes, reads, state, w_out, gain, sent, states, scratch):
    fresh, decay_rows, read_rows, sems = scratch
    read_rows[...] = reads
    high, low = hi_lo(push)
    left = jnp.concatenate([high, high, low], axis=1)
    high, low = hi_lo(writes)
    right = jnp.concatenate([high, low, high], axis=0).astype(BF16)
    of = lax.broadcasted_iota(jnp.int32, left.shape, 1) % B
    left = jnp.concatenate([jnp.where(of == b, left, 0.0).astype(BF16) for b in range(B)], axis=0)
    pushed = jnp.dot(left, right, preferred_element_type=F32)
    lane = lax.broadcasted_iota(jnp.int32, (CH, B), 1)
    found = jnp.zeros((CH, B), F32)
    copies = []
    for b in range(B):
        new = decay_rows[b : b + 1, :] * state[b] + pushed[CH * b : CH * (b + 1)]
        fresh[b] = new
        total = jnp.sum(new * read_rows[b : b + 1, :], axis=1, keepdims=True)
        found = jnp.where(lane == b, total, found)
        if b % 8 == 7:
            part = pl.ds(b - 7, 8)
            copies.append(pltpu.make_async_copy(fresh.at[part], states.at[layer, part], sems.at[b // 8]))
            copies[-1].start()
    gated = (found + direct) * gate
    total = jnp.sum(gated * gated, axis=0, keepdims=True)
    high, low = hi_lo(total)
    tail = jnp.where(lax.broadcasted_iota(jnp.int32, (2, B), 0) == 0, high, low)
    tail = jnp.concatenate([tail, jnp.zeros((2, 128 - B), F32)], axis=1).astype(BF16)
    out = jnp.dot((gated * gain).T.astype(BF16), w_out[...], preferred_element_type=F32)
    for j in range(D // 128):
        sent[LINES * j : LINES * j + B] = out[:, 128 * j : 128 * j + 128].astype(BF16)
        sent[LINES * j + B : LINES * (j + 1)] = tail
    for copy in copies:
        copy.wait()


STATES = ((2, B, CH, N), F32)
ADVANCE = (STATE, ((B, N), F32), ((B, N), F32))


def advance_scratch():
    return [pltpu.VMEM(*p) for p in ADVANCE] + [pltpu.SemaphoreType.DMA((4,))]


PLANE_SUMS = ((32 * LINES, 128), BF16)


def first_mix_kernel(keys, packed, decay, state, w_out, states, sent, weights, later, last_taps, lines, *scratch):
    lines[...] = keys[...].astype(F32)
    weights[0] = lines[pl.ds(0, N, stride=4), :].astype(BF16)
    weights[1] = lines[pl.ds(1, N, stride=4), :].astype(BF16)
    first = lines[pl.ds(2, N, stride=4), :].T
    second = lines[pl.ds(3, N, stride=4), :].T
    later[0] = first[2 * B : 3 * B]
    later[1] = first[3 * B :]
    last_taps[...] = second[2 * B : 2 * B + 8]
    writes = first[:B] + second[:B]
    reads = first[B : 2 * B] + second[B : 2 * B]
    scratch[1][...] = decay[...]
    advance(
        0, packed[0], packed[1], packed[2], writes, reads, state, w_out, packed[3], sent, states, scratch
    )


def first_mix(keys, packed, decay, kept):
    return call(
        first_mix_kernel,
        "mix0",
        [keys, packed, decay, *kept],
        [],
        [
            pltpu.HBM(*STATES),
            pltpu.VMEM(*PLANE_SUMS),
            pltpu.VMEM((2, N, 128), BF16),
            pltpu.VMEM((2, B, N), F32),
            pltpu.VMEM((8, N), F32),
        ],
        [pltpu.VMEM((4 * N, 128), F32)] + advance_scratch(),
    )


def take_half(half, side, norm_gain, weights, scaled, squares, sums):
    for at in range(16):
        cols = pl.ds(pl.multiple_of(128 * (2 * at + side), 128), 128)
        part = half[at, :B].astype(F32)
        squares += part * part
        scaled[:, 128 * at : 128 * at + 128] = (part * norm_gain[1:, cols]).astype(BF16)
        for kind in range(2):
            sums[kind] += half[at, B * (kind + 1) : B * (kind + 2)].astype(F32)
    return squares, sums, dot_nt(weights[side], scaled[...])


def half_kernel(own, weights, norm_gain, found_out, squares_out, sums_out, scaled):
    zero = jnp.zeros((B, N), F32)
    squares, sums, found = take_half(own, lax.axis_index("c"), norm_gain, weights, scaled, zero, [zero, zero])
    found_out[...] = found
    squares_out[...] = squares
    sums_out[0] = sums[0]
    sums_out[1] = sums[1]


HALF = ((B, D // 2), BF16)


def make_half(own, weights, norm_gain):
    outs = [pltpu.VMEM((ROWS, B), F32), pltpu.VMEM((B, N), F32), pltpu.VMEM((2, B, N), F32)]
    return call(half_kernel, "half", [own, weights, norm_gain], [], outs, [pltpu.VMEM(*HALF)])


def next_mix_kernel(other, weights, norm_gain, found, squares, sums, ready, later, last_taps, state, w_out, *refs):
    conv, key_conv, key_before, value_before = refs[:4]
    states, sent, key_out, value_out, scaled, *scratch = refs[5:]
    squares, sums, rest = take_half(
        other, 1 - lax.axis_index("c"), norm_gain, weights, scaled, squares[...], [sums[0], sums[1]]
    )
    inv = lax.rsqrt(jnp.sum(squares, axis=1, keepdims=True) / D + EPS)
    found = (found[...] + rest) * as_row(inv)
    keys = [silu(later[k] + sums[k] * inv * (last_taps[2 * k : 2 * k + 1] + last_taps[2 * k + 1 : 2 * k + 2])) for k in range(2)]
    fresh_values = found[CH : 2 * CH]
    values = silu(ready[0] + fresh_values * ready[1])
    delta, decay = steps_of(found[2 * CH : 2 * CH + 1] + ready[3, :1], ready[3, 1:2])
    scratch[1][...] = jnp.broadcast_to(as_col(decay), (B, N))
    direct = ready[3, 2:3] * values
    advance(
        1, delta * values, direct, silu(found[:CH]), keys[0], keys[1], state, w_out, ready[2], sent, states, scratch
    )
    value_out[0] = value_before[...]
    value_out[1, :, 0, :] = conv[1, :, 1, :]
    value_out[1, :, 1, :] = fresh_values.T
    key_out[0] = key_before[...]
    for kind in range(2):
        key_out[1, 0, kind] = key_conv[1, 1, kind]
        key_out[1, 1, kind] = found[2 * CH + 8 + 4 * kind : 2 * CH + 12 + 4 * kind]


def next_mix(near, states):
    return call(
        next_mix_kernel,
        "mix1",
        near,
        [states],
        [
            pltpu.HBM(*STATES),
            pltpu.VMEM(*PLANE_SUMS),
            shaped((2, 2, 2, 4, B), F32),
            shaped((2, B, 2, CH), F32),
        ],
        [pltpu.VMEM(*HALF)] + advance_scratch(),
        {len(near): 0},
    )


def scale_kernel(got, sent):
    total = got[:B].astype(F32)
    squares = got[B:LINES].astype(F32)
    for j in range(1, 32):
        total += got[LINES * j : LINES * j + B].astype(F32)
        squares += got[LINES * j + B : LINES * (j + 1)].astype(F32)
    squares = squares[:1, :B] + squares[1:, :B]
    factor = as_col(lax.rsqrt(squares / GW + EPS))
    chunk = (total * factor).astype(BF16)
    for plane in range(8):
        sent[plane] = chunk


def make_scale(got):
    return call(scale_kernel, "scale", [got], [], [pltpu.VMEM((8, B, 128), BF16)])[0]


def first_add_kernel(got, hid, norm_gain, weights, sent):
    total = got[0].astype(F32)
    for plane in range(1, 8):
        total += got[plane].astype(F32)
    cols = pl.ds(pl.multiple_of(128 * lax.axis_index(PLANE), 128), 128)
    chunk = (hid[:, cols].astype(F32) + total).astype(BF16)
    scaled = (chunk.astype(F32) * norm_gain[1:, cols]).astype(BF16)
    shares = [dot_nt(scaled, weights[kind]).astype(BF16) for kind in range(2)]
    for j in range(16):
        sent[j, :B] = chunk
        sent[j, B : 2 * B] = shares[0]
        sent[j, 2 * B :] = shares[1]


def next_add_kernel(got, hid, sent):
    total = got[0].astype(F32)
    for plane in range(1, 8):
        total += got[plane].astype(F32)
    chunk = (hid[lax.axis_index(("y", "x")), :B].astype(F32) + total).astype(BF16)
    for j in range(32):
        sent[j] = chunk


def exchange(value, axes):
    return lax.all_to_all(value, axes, split_axis=0, concat_axis=0, tiled=True)


def swap(value):
    return lax.ppermute(value, "c", [(0, 1), (1, 0)])


def per_device(
    tokens,
    norm_gain,
    w_gate,
    w_value,
    w_write,
    w_read,
    w_step,
    step_bias,
    decay_rate,
    skip_gain,
    conv_value_weight,
    conv_key_weight,
    group_gain,
    w_out,
    ssm_state,
    conv_value,
    conv_key,
):
    w_gate, w_value, w_write, w_read = (jnp.swapaxes(w, 1, 2) for w in (w_gate, w_value, w_write, w_read))
    conv_key = jnp.transpose(conv_key, (0, 2, 3, 4, 1))
    value_taps = jnp.swapaxes(conv_value_weight, 0, 1)
    far = [w_gate, w_value, w_step, w_write, w_read, ssm_state, w_out, group_gain, norm_gain]
    far += [step_bias, decay_rate, skip_gain, conv_value, value_taps, conv_key]
    key_far = [w_write, w_read, conv_key, conv_key_weight]
    others = [swap(v) for v in key_far]
    scaled, inv, hid, *own = make_start(tokens, norm_gain, key_far)
    msg, key_out = make_keys(scaled, inv, own, others)
    keys = exchange(msg, ("z", "y", "x")).reshape(4 * N, 128)
    packed, decay, value_out, halves, ready, *kept = make_values(scaled, inv, far)
    state, out, gain, next_state, next_out, *rest = kept
    states, sent, weights, later, last_taps = first_mix(keys, packed, decay, [state, out])
    sent = make_scale(exchange(sent.reshape(32, LINES // 2, 2, 128), PLANE).reshape(sent.shape))
    (sent,) = call(
        first_add_kernel,
        "add0",
        [exchange(sent, ("z",)), hid, rest[0], weights],
        [],
        [pltpu.VMEM((16, 3 * B, 128), BF16)],
    )
    own = exchange(sent, ("y", "x"))
    other = swap(own)
    norm_far, conv, key_conv = rest[0], rest[4], rest[6]
    half = make_half(own, halves, norm_far)
    near = [other, halves, norm_far, *half, ready, later, last_taps, next_state, next_out]
    states, sent, key_out, value_out = next_mix([*near, conv, key_conv, key_out, value_out], states)
    sent = make_scale(exchange(sent.reshape(32, LINES // 2, 2, 128), PLANE).reshape(sent.shape))
    (sent,) = call(next_add_kernel, "add1", [exchange(sent, ("z",)), own], [], [pltpu.VMEM((32, B, 128), BF16)])
    hid = exchange(sent, PLANE)
    tokens_out = jnp.transpose(hid, (1, 0, 2)).reshape(B, D)
    return (tokens_out, states, value_out, jnp.transpose(key_out, (0, 4, 1, 2, 3)))


def solution(mesh):
    torus = Mesh(mesh.devices.reshape(8, 4, 4, 2), TP)
    in_specs = (
        P(),
        P(),
        P(None, None, TP),
        P(None, None, TP),
        P(None, None, TP),
        P(None, None, TP),
        P(),
        P(),
        P(),
        P(),
        P(None, None, TP),
        P(None, None, None, TP),
        P(None, TP),
        P(None, TP, None),
        P(None, None, TP, None),
        P(None, None, None, TP),
        P(None, None, None, None, TP),
    )
    out_specs = (
        P(),
        P(None, None, TP, None),
        P(None, None, None, TP),
        P(None, None, None, None, TP),
    )
    return jax.shard_map(
        per_device, mesh=torus, in_specs=in_specs, out_specs=out_specs, check_vma=False
    )
```

```python
import functools

import jax
import jax.numpy as jnp
from jax import lax
from jax.experimental import pallas as pl
from jax.experimental.pallas import tpu as pltpu
from jax.sharding import Mesh
from jax.sharding import PartitionSpec as P

D = 4096
B = 32
CH = 32
N = 128
GW = 1024
LINES = B + 2
FIRST_SPOT = 64
FIRST_MEMBER = 1
FIRST_PLANE = 4
FIRST_CHIP = 0
LAST_MEMBER = 21
EPS = 1e-06
TP = ("z", "y", "x", "c")
PLANE = ("y", "x", "c")
F32 = jnp.float32
BF16 = jnp.bfloat16


LIMIT = pltpu.CompilerParams(vmem_limit_bytes=8 * 1024 * 1024)


def vmem():
    return pl.BlockSpec(memory_space=pltpu.VMEM)


def anywhere():
    return pl.BlockSpec(memory_space=pl.ANY)


def shaped(shape, dtype):
    return jax.ShapeDtypeStruct(shape, dtype)


def start_all(pairs, sems):
    copies = [pltpu.make_async_copy(src, dst, sems.at[at]) for at, (src, dst) in enumerate(pairs)]
    for copy in copies:
        copy.start()
    return copies


def call(body, name, near, far, outs, scratch=(), aliases=None):
    near = [pltpu.with_memory_space_constraint(v, pltpu.VMEM) for v in near]
    far = [pltpu.with_memory_space_constraint(v, pltpu.HBM) for v in far]
    far_out = (pltpu.HBM((1,), F32).memory_space,)
    specs = [anywhere() if getattr(o, "memory_space", None) in far_out else vmem() for o in outs]
    return pl.pallas_call(
        body,
        in_specs=[vmem()] * len(near) + [anywhere()] * len(far),
        out_specs=specs,
        out_shape=list(outs),
        scratch_shapes=list(scratch),
        input_output_aliases=aliases or {},
        compiler_params=LIMIT,
        name=name,
    )(*near, *far)


def silu(v):
    return v / (1.0 + jnp.exp(-v))


def as_col(row):
    n = row.shape[1]
    at = lax.broadcasted_iota(jnp.int32, (n, n), 0)
    of = lax.broadcasted_iota(jnp.int32, (n, n), 1)
    return jnp.sum(jnp.where(at == of, row, 0.0), axis=1, keepdims=True)


def as_row(col):
    n = col.shape[0]
    at = lax.broadcasted_iota(jnp.int32, (n, n), 0)
    of = lax.broadcasted_iota(jnp.int32, (n, n), 1)
    return jnp.sum(jnp.where(at == of, col, 0.0), axis=0, keepdims=True)


def dot_nt(a, b):
    return lax.dot_general(a, b, (((1,), (1,)), ((), ())), preferred_element_type=F32)


def hi_lo(value):
    high = value.astype(BF16).astype(F32)
    return high, value - high


def scale_tokens(part_of, gain, scaled):
    squares = jnp.zeros((B, 128), F32)
    for j in range(D // 128):
        cols = slice(128 * j, 128 * j + 128)
        part = part_of(j).astype(F32)
        squares += part * part
        scaled[:, cols] = (part * gain[:, cols]).astype(BF16)
    return lax.rsqrt(jnp.sum(squares, axis=1, keepdims=True) / D + EPS)


KEY_WEIGHTS = ((4, D), BF16)
KEY_PARAMS = (((2, 4, D), BF16), ((2, 4, D), BF16), ((2, 2, 2, 4, B), F32), ((2, 3, 2, 4), F32))


def start_kernel(tokens, gain_far, *refs):
    far, (scaled, inv_out, hid), near, (gain, sems, late_sems) = refs[:4], refs[4:7], refs[7:11], refs[11:]
    copies = start_all([(tokens, hid), (gain_far, gain)], sems)
    late = start_all(list(zip(far, near)), late_sems)
    for copy in copies:
        copy.wait()
    inv = scale_tokens(lambda j: hid[:, 128 * j : 128 * j + 128], gain.at[:1], scaled)
    inv_out[...] = jnp.broadcast_to(inv, (B, 128))
    for copy in late:
        copy.wait()


def make_start(tokens, gain, far):
    outs = [((B, D), BF16), ((B, 128), F32), ((B, D), BF16), *KEY_PARAMS]
    return call(
        start_kernel,
        "start",
        [],
        [tokens, gain, *far],
        [pltpu.VMEM(*p) for p in outs],
        [pltpu.VMEM((2, D), F32), pltpu.SemaphoreType.DMA((2,)), pltpu.SemaphoreType.DMA((4,))],
    )


def keys_kernel(scaled, inv, *refs):
    sides, (msg, conv_out) = (refs[:4], refs[4:8]), refs[8:]
    core = lax.axis_index("c")
    rows = [weight[0].astype(F32) for side in sides for weight in side[:2]]
    found = dot_nt(jnp.concatenate(rows, axis=0).astype(BF16), scaled[...]) * as_row(inv[:, :1])
    lane = lax.broadcasted_iota(jnp.int32, (4, B), 1)
    row = lax.broadcasted_iota(jnp.int32, (4, 128), 0)
    for of, (w_write, w_read, conv, taps) in enumerate(sides):
        mixed, later, last_taps = [], [], []
        for kind in range(2):
            at = 8 * of + 4 * kind
            fresh = found[at : at + 4]
            old, newer = conv[0, 0, kind], conv[0, 1, kind]
            tap = [[as_col(taps[layer, k, kind : kind + 1, :]) for k in range(3)] for layer in range(2)]
            mixed.append(silu(old * tap[0][0] + newer * tap[0][1] + fresh * tap[0][2]))
            later.append(conv[1, 0, kind] * tap[1][0] + conv[1, 1, kind] * tap[1][1])
            last_taps.append(tap[1][2])
            if not of:
                conv_out[0, kind] = newer
                conv_out[1, kind] = fresh
        mixed_hi, mixed_lo = zip(*(hi_lo(v) for v in mixed))
        taps_hi, taps_lo = zip(*(hi_lo(v) for v in last_taps))
        first = jnp.concatenate([*mixed_hi, *later], axis=1)
        tail = jnp.zeros((4, B), F32)
        for at, col in enumerate((taps_hi[0], taps_lo[0], taps_hi[1], taps_lo[1])):
            tail = jnp.where(lane == at, col, tail)
        second = jnp.concatenate([*mixed_lo, tail, jnp.zeros((4, B), F32)], axis=1)
        base = [jnp.where(row == 2, first[col : col + 1], second[col : col + 1]) for col in range(4)]
        side = 1 - core if of else core
        start = 64 * (1 - side if FIRST_SPOT & 64 else side)
        for place in range(16):
            cols = pl.ds(pl.multiple_of(128 * (2 * place + core), 128), 128)
            writes = w_write[1, :, cols].astype(F32)
            reads = w_read[1, :, cols].astype(F32)
            for col in range(4):
                one = slice(col, col + 1)
                tile = jnp.where(row == 0, writes[one], jnp.where(row == 1, reads[one], base[col]))
                msg[start + ((16 * col + place) ^ (FIRST_SPOT & 63))] = tile.astype(BF16)


def make_keys(scaled, inv, own, other):
    return call(
        keys_kernel,
        "keys",
        [scaled, inv, *own, *other],
        [],
        [shaped((128, 4, 128), BF16), pltpu.VMEM((2, 2, 4, B), F32)],
    )


def of_head(table):
    head = lax.axis_index(("z", "y", "x"))
    mine = lax.broadcasted_iota(jnp.int32, (1, 128), 1) == head
    return jnp.sum(jnp.where(mine, table, 0.0), axis=1, keepdims=True)


def steps_of(raw, rate):
    delta = jnp.maximum(raw, 0.0) + jnp.log1p(jnp.exp(-jnp.abs(raw)))
    return delta, jnp.exp(-delta * rate)


def row_of(table, layer):
    return table[layer : layer + 1, :]


STATE = ((B, CH, N), F32)
OUT = ((CH, D), BF16)
ROWS = 80
NOW_FAR = (((CH, D), BF16), ((CH, D), BF16), ((D, 128), BF16))
NEXT_FAR = (((D, 128), BF16), KEY_WEIGHTS, KEY_WEIGHTS)
KEPT = (
    STATE,
    OUT,
    ((2, CH), F32),
    STATE,
    OUT,
    ((2, D), F32),
    ((2, 128), F32),
    ((2, 128), F32),
    ((2, 128), F32),
    ((2, B, 2, CH), F32),
    ((3, 2, CH), F32),
    ((2, 2, 2, 4, B), F32),
)


def values_kernel(scaled, inv, *refs):
    far, refs = refs[:15], refs[15:]
    packed, decay_out, conv_out, halves, ready, *kept = refs[: 5 + len(KEPT)]
    w_gate, w_value, w_step, next_step, next_write, next_read, stack, sems, late_sems = refs[5 + len(KEPT) :]
    gate_far, value_far, step_far, write_far, read_far, state_far, out_far, *tables_far = far
    tables_group, tables_rest = tables_far[0], tables_far[1:]
    late_sources = [
        state_far.at[0], out_far.at[0], tables_group, state_far.at[1], out_far.at[1], *tables_rest
    ]
    late = list(zip(late_sources, kept))
    small = [(src, dst) for src, dst in late[6:11]]
    now = [(gate_far.at[0], w_gate), (value_far.at[0], w_value), (step_far.at[0], w_step)] + small
    copies = start_all(now, sems)
    late = late[:6] + late[11:]
    late += [
        (gate_far.at[1], stack.at[:CH]),
        (value_far.at[1], stack.at[CH : 2 * CH]),
        (step_far.at[1], next_step),
        (write_far.at[1], next_write),
        (read_far.at[1], next_read),
    ]
    late = start_all(late, late_sems)
    for copy in copies:
        copy.wait()
    hidden = scaled[...]
    inv_col = inv[:, :CH]
    gate = dot_nt(hidden, w_gate[...]) * inv_col
    fresh = dot_nt(hidden, w_value[...]) * inv_col
    raw = of_head(jnp.dot(hidden, w_step[...], preferred_element_type=F32) * inv[...])
    (bias, rate, skip), conv, taps = kept[6:9], kept[9], kept[10]
    tap = [[row_of(taps[k], layer) for k in range(3)] for layer in range(2)]
    values = silu(conv[0, :, 0, :] * tap[0][0] + conv[0, :, 1, :] * tap[0][1] + fresh * tap[0][2])
    delta, decay = steps_of(raw + of_head(row_of(bias, 0)), of_head(row_of(rate, 0)))
    packed[0] = (delta * values).T
    packed[1] = (of_head(row_of(skip, 0)) * values).T
    packed[2] = silu(gate).T
    decay_out[...] = jnp.broadcast_to(decay, (B, N))
    conv_out[:, 0, :] = conv[0, :, 1, :]
    conv_out[:, 1, :] = fresh
    for copy in late:
        copy.wait()
    head = lax.axis_index(("z", "y", "x"))
    hot = (lax.broadcasted_iota(jnp.int32, (8, 128), 1) == head).astype(F32).astype(BF16)
    stack[2 * CH : 2 * CH + 8] = dot_nt(hot, next_step[...]).astype(BF16)
    both = jnp.concatenate([next_write[...].astype(F32), next_read[...].astype(F32)], axis=0)
    stack[2 * CH + 8 :] = both.astype(BF16)
    for place in range(16):
        for side in range(2):
            at = 128 * (2 * (place ^ FIRST_CHIP) + side)
            halves[side, :, 128 * place : 128 * place + 128] = stack[:, at : at + 128]
    packed[3] = jnp.broadcast_to(as_col(row_of(kept[2], 0)), (CH, B))
    ready[0] = (conv[1, :, 0, :] * tap[1][0] + conv[1, :, 1, :] * tap[1][1]).T
    ready[1] = jnp.broadcast_to(as_col(tap[1][2]), (CH, B))
    ready[2] = jnp.broadcast_to(as_col(row_of(kept[2], 1)), (CH, B))
    for at, table in enumerate((bias, rate, skip)):
        ready[3, at : at + 1] = jnp.broadcast_to(of_head(row_of(table, 1)), (1, B))


def make_values(scaled, inv, far):
    outs = [pltpu.VMEM((4, CH, B), F32), pltpu.VMEM((B, N), F32)]
    outs += [pltpu.VMEM((B, 2, CH), F32), pltpu.VMEM((2, ROWS, D // 2), BF16), pltpu.VMEM((4, CH, B), F32)]
    outs += [pltpu.VMEM(*p) for p in KEPT]
    scratch = [pltpu.VMEM(*p) for p in (*NOW_FAR, *NEXT_FAR, ((ROWS, D), BF16))]
    scratch += [pltpu.SemaphoreType.DMA((8,)), pltpu.SemaphoreType.DMA((12,))]
    return call(values_kernel, "values", [scaled, inv], far, outs, scratch)


def advance(layer, push, direct, gate, writes, reads, state, w_out, gain, sent, states, scratch):
    fresh, decay_rows, read_rows, sems = scratch
    read_rows[...] = reads
    high, low = hi_lo(push)
    left = jnp.concatenate([high, high, low], axis=1)
    high, low = hi_lo(writes)
    right = jnp.concatenate([high, low, high], axis=0).astype(BF16)
    of = lax.broadcasted_iota(jnp.int32, left.shape, 1) % B
    left = jnp.concatenate([jnp.where(of == b, left, 0.0).astype(BF16) for b in range(B)], axis=0)
    pushed = jnp.dot(left, right, preferred_element_type=F32)
    lane = lax.broadcasted_iota(jnp.int32, (CH, B), 1)
    found = jnp.zeros((CH, B), F32)
    copies = []
    for b in range(B):
        new = decay_rows[b : b + 1, :] * state[b] + pushed[CH * b : CH * (b + 1)]
        fresh[b] = new
        total = jnp.sum(new * read_rows[b : b + 1, :], axis=1, keepdims=True)
        found = jnp.where(lane == b, total, found)
        if b % 8 == 7:
            part = pl.ds(b - 7, 8)
            copies.append(pltpu.make_async_copy(fresh.at[part], states.at[layer, part], sems.at[b // 8]))
            copies[-1].start()
    gated = (found + direct) * gate
    total = jnp.sum(gated * gated, axis=0, keepdims=True)
    high, low = hi_lo(total)
    tail = jnp.where(lax.broadcasted_iota(jnp.int32, (2, B), 0) == 0, high, low)
    tail = jnp.concatenate([tail, jnp.zeros((2, 128 - B), F32)], axis=1).astype(BF16)
    out = jnp.dot((gated * gain).T.astype(BF16), w_out[...], preferred_element_type=F32)
    for j in range(D // 128):
        to = LINES * (j ^ FIRST_MEMBER)
        sent[to : to + B] = out[:, 128 * j : 128 * j + 128].astype(BF16)
        sent[to + B : to + LINES] = tail
    for copy in copies:
        copy.wait()


STATES = ((2, B, CH, N), F32)
ADVANCE = (STATE, ((B, N), F32), ((B, N), F32))


def advance_scratch():
    return [pltpu.VMEM(*p) for p in ADVANCE] + [pltpu.SemaphoreType.DMA((4,))]


PLANE_SUMS = ((32 * LINES, 128), BF16)


def first_mix_kernel(keys, packed, decay, state, w_out, states, sent, weights, later, last_taps, lines, *scratch):
    for at in range(0, 4 * N, 16):
        pair = keys[at : at + 16].astype(F32)
        for half in range(2):
            to = (at + 8 * half) ^ (4 * FIRST_SPOT)
            lines[to : to + 8] = pair[8 * half : 8 * half + 8]
    weights[0] = lines[pl.ds(0, N, stride=4), :].astype(BF16)
    weights[1] = lines[pl.ds(1, N, stride=4), :].astype(BF16)
    first = lines[pl.ds(2, N, stride=4), :].T
    second = lines[pl.ds(3, N, stride=4), :].T
    later[0] = first[2 * B : 3 * B]
    later[1] = first[3 * B :]
    last_taps[...] = second[2 * B : 2 * B + 8]
    writes = first[:B] + second[:B]
    reads = first[B : 2 * B] + second[B : 2 * B]
    scratch[1][...] = decay[...]
    advance(
        0, packed[0], packed[1], packed[2], writes, reads, state, w_out, packed[3], sent, states, scratch
    )


def first_mix(keys, packed, decay, kept):
    return call(
        first_mix_kernel,
        "mix0",
        [keys, packed, decay, *kept],
        [],
        [
            pltpu.HBM(*STATES),
            pltpu.VMEM(*PLANE_SUMS),
            pltpu.VMEM((2, N, 128), BF16),
            pltpu.VMEM((2, B, N), F32),
            pltpu.VMEM((8, N), F32),
        ],
        [pltpu.VMEM((4 * N, 128), F32)] + advance_scratch(),
    )


def take_half(half, side, norm_gain, weights, scaled, squares, sums):
    for at in range(16):
        cols = pl.ds(pl.multiple_of(128 * (2 * (at ^ FIRST_CHIP) + side), 128), 128)
        part = half[at, :B].astype(F32)
        squares += part * part
        scaled[:, 128 * at : 128 * at + 128] = (part * norm_gain[1:, cols]).astype(BF16)
        for kind in range(2):
            sums[kind] += half[at, B * (kind + 1) : B * (kind + 2)].astype(F32)
    return squares, sums, dot_nt(weights[side], scaled[...])


def half_kernel(own, weights, norm_gain, found_out, squares_out, sums_out, scaled):
    zero = jnp.zeros((B, N), F32)
    squares, sums, found = take_half(own, lax.axis_index("c"), norm_gain, weights, scaled, zero, [zero, zero])
    found_out[...] = found
    squares_out[...] = squares
    sums_out[0] = sums[0]
    sums_out[1] = sums[1]


HALF = ((B, D // 2), BF16)


def make_half(own, weights, norm_gain):
    outs = [pltpu.VMEM((ROWS, B), F32), pltpu.VMEM((B, N), F32), pltpu.VMEM((2, B, N), F32)]
    return call(half_kernel, "half", [own, weights, norm_gain], [], outs, [pltpu.VMEM(*HALF)])


def next_mix_kernel(other, weights, norm_gain, found, squares, sums, ready, later, last_taps, state, w_out, *refs):
    conv, key_conv, key_before, value_before = refs[:4]
    states, sent, key_out, value_out, scaled, *scratch = refs[5:]
    squares, sums, rest = take_half(
        other, 1 - lax.axis_index("c"), norm_gain, weights, scaled, squares[...], [sums[0], sums[1]]
    )
    inv = lax.rsqrt(jnp.sum(squares, axis=1, keepdims=True) / D + EPS)
    found = (found[...] + rest) * as_row(inv)
    keys = [silu(later[k] + sums[k] * inv * (last_taps[2 * k : 2 * k + 1] + last_taps[2 * k + 1 : 2 * k + 2])) for k in range(2)]
    fresh_values = found[CH : 2 * CH]
    values = silu(ready[0] + fresh_values * ready[1])
    delta, decay = steps_of(found[2 * CH : 2 * CH + 1] + ready[3, :1], ready[3, 1:2])
    scratch[1][...] = jnp.broadcast_to(as_col(decay), (B, N))
    direct = ready[3, 2:3] * values
    advance(
        1, delta * values, direct, silu(found[:CH]), keys[0], keys[1], state, w_out, ready[2], sent, states, scratch
    )
    value_out[0] = value_before[...]
    value_out[1, :, 0, :] = conv[1, :, 1, :]
    value_out[1, :, 1, :] = fresh_values.T
    key_out[0] = key_before[...]
    for kind in range(2):
        key_out[1, 0, kind] = key_conv[1, 1, kind]
        key_out[1, 1, kind] = found[2 * CH + 8 + 4 * kind : 2 * CH + 12 + 4 * kind]


def next_mix(near, states):
    return call(
        next_mix_kernel,
        "mix1",
        near,
        [states],
        [
            pltpu.HBM(*STATES),
            pltpu.VMEM(*PLANE_SUMS),
            shaped((2, 2, 2, 4, B), F32),
            shaped((2, B, 2, CH), F32),
        ],
        [pltpu.VMEM(*HALF)] + advance_scratch(),
        {len(near): 0},
    )


def scale_kernel(got, sent):
    total = got[:B].astype(F32)
    squares = got[B:LINES].astype(F32)
    for j in range(1, 32):
        total += got[LINES * j : LINES * j + B].astype(F32)
        squares += got[LINES * j + B : LINES * (j + 1)].astype(F32)
    squares = squares[:1, :B] + squares[1:, :B]
    factor = as_col(lax.rsqrt(squares / GW + EPS))
    chunk = (total * factor).astype(BF16)
    for plane in range(8):
        sent[plane] = chunk


def make_scale(got):
    return call(scale_kernel, "scale", [got], [], [pltpu.VMEM((8, B, 128), BF16)])[0]


def first_add_kernel(got, hid, norm_gain, weights, sent):
    total = got[0].astype(F32)
    for plane in range(1, 8):
        total += got[plane].astype(F32)
    cols = pl.ds(pl.multiple_of(128 * lax.axis_index(PLANE), 128), 128)
    chunk = (hid[:, cols].astype(F32) + total).astype(BF16)
    scaled = (chunk.astype(F32) * norm_gain[1:, cols]).astype(BF16)
    shares = [dot_nt(scaled, weights[kind]).astype(BF16) for kind in range(2)]
    for j in range(16):
        sent[j, :B] = chunk
        sent[j, B : 2 * B] = shares[0]
        sent[j, 2 * B :] = shares[1]


def next_add_kernel(got, hid, sent):
    total = got[0].astype(F32)
    for plane in range(1, 8):
        total += got[plane].astype(F32)
    chunk = (hid[lax.axis_index(("y", "x")) ^ FIRST_CHIP, :B].astype(F32) + total).astype(BF16)
    for j in range(32):
        sent[j] = chunk


def tokens_kernel(got, tokens_out):
    for j in range(32):
        at = 128 * (j ^ LAST_MEMBER)
        tokens_out[:, at : at + 128] = got[j]


def make_tokens(got):
    return call(tokens_kernel, "tokens", [got], [], [shaped((B, D), BF16)])[0]


def exchange(value, axes, first):
    order = [spot ^ first for spot in range(value.shape[0])]
    return lax.all_to_all(value, axes, 0, 0, axis_index_groups=[order], tiled=True)


def swap(value):
    return lax.ppermute(value, "c", [(0, 1), (1, 0)])


def per_device(
    tokens,
    norm_gain,
    w_gate,
    w_value,
    w_write,
    w_read,
    w_step,
    step_bias,
    decay_rate,
    skip_gain,
    conv_value_weight,
    conv_key_weight,
    group_gain,
    w_out,
    ssm_state,
    conv_value,
    conv_key,
):
    w_gate, w_value, w_write, w_read = (jnp.swapaxes(w, 1, 2) for w in (w_gate, w_value, w_write, w_read))
    conv_key = jnp.transpose(conv_key, (0, 2, 3, 4, 1))
    value_taps = jnp.swapaxes(conv_value_weight, 0, 1)
    far = [w_gate, w_value, w_step, w_write, w_read, ssm_state, w_out, group_gain, norm_gain]
    far += [step_bias, decay_rate, skip_gain, conv_value, value_taps, conv_key]
    key_far = [w_write, w_read, conv_key, conv_key_weight]
    others = [swap(v) for v in key_far]
    scaled, inv, hid, *own = make_start(tokens, norm_gain, key_far)
    msg, key_out = make_keys(scaled, inv, own, others)
    keys = exchange(msg, ("z", "y", "x"), FIRST_SPOT).reshape(4 * N, 128)
    packed, decay, value_out, halves, ready, *kept = make_values(scaled, inv, far)
    state, out, gain, next_state, next_out, *rest = kept
    states, sent, weights, later, last_taps = first_mix(keys, packed, decay, [state, out])
    sent = make_scale(exchange(sent.reshape(32, LINES // 2, 2, 128), PLANE, FIRST_MEMBER).reshape(sent.shape))
    (sent,) = call(
        first_add_kernel,
        "add0",
        [exchange(sent, ("z",), FIRST_PLANE), hid, rest[0], weights],
        [],
        [pltpu.VMEM((16, 3 * B, 128), BF16)],
    )
    own = exchange(sent, ("y", "x"), FIRST_CHIP)
    other = swap(own)
    norm_far, conv, key_conv = rest[0], rest[4], rest[6]
    half = make_half(own, halves, norm_far)
    near = [other, halves, norm_far, *half, ready, later, last_taps, next_state, next_out]
    states, sent, key_out, value_out = next_mix([*near, conv, key_conv, key_out, value_out], states)
    sent = make_scale(exchange(sent.reshape(32, LINES // 2, 2, 128), PLANE, FIRST_MEMBER).reshape(sent.shape))
    (sent,) = call(next_add_kernel, "add1", [exchange(sent, ("z",), FIRST_PLANE), own], [], [pltpu.VMEM((32, B, 128), BF16)])
    hid = exchange(sent, PLANE, LAST_MEMBER)
    tokens_out = make_tokens(hid)
    return (tokens_out, states, value_out, jnp.transpose(key_out, (0, 4, 1, 2, 3)))


def solution(mesh):
    torus = Mesh(mesh.devices.reshape(8, 4, 4, 2), TP)
    in_specs = (
        P(),
        P(),
        P(None, None, TP),
        P(None, None, TP),
        P(None, None, TP),
        P(None, None, TP),
        P(),
        P(),
        P(),
        P(),
        P(None, None, TP),
        P(None, None, None, TP),
        P(None, TP),
        P(None, TP, None),
        P(None, None, TP, None),
        P(None, None, None, TP),
        P(None, None, None, None, TP),
    )
    out_specs = (
        P(),
        P(None, None, TP, None),
        P(None, None, None, TP),
        P(None, None, None, None, TP),
    )
    return jax.shard_map(
        per_device, mesh=torus, in_specs=in_specs, out_specs=out_specs, check_vma=False
    )
```

```python
import functools

import jax
import jax.numpy as jnp
from jax import lax
from jax.experimental import pallas as pl
from jax.experimental.pallas import tpu as pltpu
from jax.sharding import Mesh
from jax.sharding import PartitionSpec as P

D = 4096
B = 32
CH = 32
N = 128
GW = 1024
LINES = B + 2
FIRST_SPOT = 64
FIRST_MEMBER = 1
FIRST_PLANE = 4
FIRST_CHIP = 0
LAST_MEMBER = 21
EPS = 1e-06
TP = ("z", "y", "x", "c")
PLANE = ("y", "x", "c")
F32 = jnp.float32
BF16 = jnp.bfloat16


LIMIT = pltpu.CompilerParams(vmem_limit_bytes=8 * 1024 * 1024)


def vmem():
    return pl.BlockSpec(memory_space=pltpu.VMEM)


def anywhere():
    return pl.BlockSpec(memory_space=pl.ANY)


def shaped(shape, dtype):
    return jax.ShapeDtypeStruct(shape, dtype)


def start_all(pairs, sems):
    copies = [pltpu.make_async_copy(src, dst, sems.at[at]) for at, (src, dst) in enumerate(pairs)]
    for copy in copies:
        copy.start()
    return copies


def call(body, name, near, far, outs, scratch=(), aliases=None):
    near = [pltpu.with_memory_space_constraint(v, pltpu.VMEM) for v in near]
    far = [pltpu.with_memory_space_constraint(v, pltpu.HBM) for v in far]
    far_out = (pltpu.HBM((1,), F32).memory_space,)
    specs = [anywhere() if getattr(o, "memory_space", None) in far_out else vmem() for o in outs]
    return pl.pallas_call(
        body,
        in_specs=[vmem()] * len(near) + [anywhere()] * len(far),
        out_specs=specs,
        out_shape=list(outs),
        scratch_shapes=list(scratch),
        input_output_aliases=aliases or {},
        compiler_params=LIMIT,
        name=name,
    )(*near, *far)


def silu(v):
    return v / (1.0 + jnp.exp(-v))


def as_col(row):
    n = row.shape[1]
    at = lax.broadcasted_iota(jnp.int32, (n, n), 0)
    of = lax.broadcasted_iota(jnp.int32, (n, n), 1)
    return jnp.sum(jnp.where(at == of, row, 0.0), axis=1, keepdims=True)


def as_row(col):
    n = col.shape[0]
    at = lax.broadcasted_iota(jnp.int32, (n, n), 0)
    of = lax.broadcasted_iota(jnp.int32, (n, n), 1)
    return jnp.sum(jnp.where(at == of, col, 0.0), axis=0, keepdims=True)


def dot_nt(a, b):
    return lax.dot_general(a, b, (((1,), (1,)), ((), ())), preferred_element_type=F32)


def hi_lo(value):
    high = value.astype(BF16).astype(F32)
    return high, value - high


def scale_tokens(part_of, gain, scaled):
    squares = jnp.zeros((B, 128), F32)
    for j in range(D // 128):
        cols = slice(128 * j, 128 * j + 128)
        part = part_of(j).astype(F32)
        squares += part * part
        scaled[:, cols] = (part * gain[:, cols]).astype(BF16)
    return lax.rsqrt(jnp.sum(squares, axis=1, keepdims=True) / D + EPS)


KEY_WEIGHTS = ((4, D), BF16)
KEY_PARAMS = (((2, 4, D), BF16), ((2, 4, D), BF16), ((2, 2, 2, 4, B), F32), ((2, 3, 2, 4), F32))


def start_kernel(tokens, gain_far, *refs):
    far, (scaled, inv_out, hid), near, (gain, sems, late_sems) = refs[:4], refs[4:7], refs[7:11], refs[11:]
    copies = start_all([(tokens, hid), (gain_far, gain)], sems)
    late = start_all(list(zip(far, near)), late_sems)
    for copy in copies:
        copy.wait()
    inv = scale_tokens(lambda j: hid[:, 128 * j : 128 * j + 128], gain.at[:1], scaled)
    inv_out[...] = jnp.broadcast_to(inv, (B, 128))
    for copy in late:
        copy.wait()


def make_start(tokens, gain, far):
    outs = [((B, D), BF16), ((B, 128), F32), ((B, D), BF16), *KEY_PARAMS]
    return call(
        start_kernel,
        "start",
        [],
        [tokens, gain, *far],
        [pltpu.VMEM(*p) for p in outs],
        [pltpu.VMEM((2, D), F32), pltpu.SemaphoreType.DMA((2,)), pltpu.SemaphoreType.DMA((4,))],
    )


def keys_kernel(scaled, inv, *refs):
    sides, (msg, conv_out) = (refs[:4], refs[4:8]), refs[8:]
    core = lax.axis_index("c")
    rows = [weight[0].astype(F32) for side in sides for weight in side[:2]]
    found = dot_nt(jnp.concatenate(rows, axis=0).astype(BF16), scaled[...]) * as_row(inv[:, :1])
    lane = lax.broadcasted_iota(jnp.int32, (4, B), 1)
    row = lax.broadcasted_iota(jnp.int32, (4, 128), 0)
    for of, (w_write, w_read, conv, taps) in enumerate(sides):
        mixed, later, last_taps = [], [], []
        for kind in range(2):
            at = 8 * of + 4 * kind
            fresh = found[at : at + 4]
            old, newer = conv[0, 0, kind], conv[0, 1, kind]
            tap = [[as_col(taps[layer, k, kind : kind + 1, :]) for k in range(3)] for layer in range(2)]
            mixed.append(silu(old * tap[0][0] + newer * tap[0][1] + fresh * tap[0][2]))
            later.append(conv[1, 0, kind] * tap[1][0] + conv[1, 1, kind] * tap[1][1])
            last_taps.append(tap[1][2])
            if not of:
                conv_out[0, kind] = newer
                conv_out[1, kind] = fresh
        mixed_hi, mixed_lo = zip(*(hi_lo(v) for v in mixed))
        taps_hi, taps_lo = zip(*(hi_lo(v) for v in last_taps))
        first = jnp.concatenate([*mixed_hi, *later], axis=1)
        tail = jnp.zeros((4, B), F32)
        for at, col in enumerate((taps_hi[0], taps_lo[0], taps_hi[1], taps_lo[1])):
            tail = jnp.where(lane == at, col, tail)
        second = jnp.concatenate([*mixed_lo, tail, jnp.zeros((4, B), F32)], axis=1)
        base = [jnp.where(row == 2, first[col : col + 1], second[col : col + 1]) for col in range(4)]
        side = 1 - core if of else core
        start = 64 * (1 - side if FIRST_SPOT & 64 else side)
        for place in range(16):
            cols = pl.ds(pl.multiple_of(128 * (2 * place + core), 128), 128)
            writes = w_write[1, :, cols].astype(F32)
            reads = w_read[1, :, cols].astype(F32)
            for col in range(4):
                one = slice(col, col + 1)
                tile = jnp.where(row == 0, writes[one], jnp.where(row == 1, reads[one], base[col]))
                msg[start + ((16 * col + place) ^ (FIRST_SPOT & 63))] = tile.astype(BF16)


def make_keys(scaled, inv, own, other):
    return call(
        keys_kernel,
        "keys",
        [scaled, inv, *own, *other],
        [],
        [shaped((128, 4, 128), BF16), pltpu.VMEM((2, 2, 4, B), F32)],
    )


def of_head(table):
    head = lax.axis_index(("z", "y", "x"))
    mine = lax.broadcasted_iota(jnp.int32, (1, 128), 1) == head
    return jnp.sum(jnp.where(mine, table, 0.0), axis=1, keepdims=True)


def steps_of(raw, rate):
    delta = jnp.maximum(raw, 0.0) + jnp.log1p(jnp.exp(-jnp.abs(raw)))
    return delta, jnp.exp(-delta * rate)


def row_of(table, layer):
    return table[layer : layer + 1, :]


STATE = ((B, CH, N), F32)
OUT = ((CH, D), BF16)
ROWS = 80
NOW_FAR = (((CH, D), BF16), ((CH, D), BF16), ((D, 128), BF16))
NEXT_FAR = (((D, 128), BF16), KEY_WEIGHTS, KEY_WEIGHTS)
KEPT = (
    STATE,
    OUT,
    ((2, CH), F32),
    STATE,
    OUT,
    ((2, D), F32),
    ((2, 128), F32),
    ((2, 128), F32),
    ((2, 128), F32),
    ((2, B, 2, CH), F32),
    ((3, 2, CH), F32),
    ((2, 2, 2, 4, B), F32),
)


def values_kernel(scaled, inv, *refs):
    far, refs = refs[:15], refs[15:]
    packed, decay_out, conv_out, halves, ready, *kept = refs[: 5 + len(KEPT)]
    w_gate, w_value, w_step, next_step, next_write, next_read, stack, sems, late_sems = refs[5 + len(KEPT) :]
    gate_far, value_far, step_far, write_far, read_far, state_far, out_far, *tables_far = far
    tables_group, tables_rest = tables_far[0], tables_far[1:]
    late_sources = [
        state_far.at[0], out_far.at[0], tables_group, state_far.at[1], out_far.at[1], *tables_rest
    ]
    late = list(zip(late_sources, kept))
    small = [(src, dst) for src, dst in late[6:11]]
    now = [(gate_far.at[0], w_gate), (value_far.at[0], w_value), (step_far.at[0], w_step)] + small
    copies = start_all(now, sems)
    late = late[:6] + late[11:]
    late += [
        (gate_far.at[1], stack.at[:CH]),
        (value_far.at[1], stack.at[CH : 2 * CH]),
        (step_far.at[1], next_step),
        (write_far.at[1], next_write),
        (read_far.at[1], next_read),
    ]
    late = start_all(late, late_sems)
    for copy in copies:
        copy.wait()
    hidden = scaled[...]
    inv_col = inv[:, :CH]
    gate = dot_nt(hidden, w_gate[...]) * inv_col
    fresh = dot_nt(hidden, w_value[...]) * inv_col
    raw = of_head(jnp.dot(hidden, w_step[...], preferred_element_type=F32) * inv[...])
    (bias, rate, skip), conv, taps = kept[6:9], kept[9], kept[10]
    tap = [[row_of(taps[k], layer) for k in range(3)] for layer in range(2)]
    values = silu(conv[0, :, 0, :] * tap[0][0] + conv[0, :, 1, :] * tap[0][1] + fresh * tap[0][2])
    delta, decay = steps_of(raw + of_head(row_of(bias, 0)), of_head(row_of(rate, 0)))
    packed[0] = (delta * values).T
    packed[1] = (of_head(row_of(skip, 0)) * values).T
    packed[2] = silu(gate).T
    decay_out[...] = jnp.broadcast_to(decay, (B, N))
    conv_out[:, 0, :] = conv[0, :, 1, :]
    conv_out[:, 1, :] = fresh
    for copy in late:
        copy.wait()
    head = lax.axis_index(("z", "y", "x"))
    hot = (lax.broadcasted_iota(jnp.int32, (8, 128), 1) == head).astype(F32).astype(BF16)
    stack[2 * CH : 2 * CH + 8] = dot_nt(hot, next_step[...]).astype(BF16)
    both = jnp.concatenate([next_write[...].astype(F32), next_read[...].astype(F32)], axis=0)
    stack[2 * CH + 8 :] = both.astype(BF16)
    for place in range(16):
        for side in range(2):
            at = 128 * (2 * (place ^ FIRST_CHIP) + side)
            halves[side, :, 128 * place : 128 * place + 128] = stack[:, at : at + 128]
    packed[3] = jnp.broadcast_to(as_col(row_of(kept[2], 0)), (CH, B))
    ready[0] = (conv[1, :, 0, :] * tap[1][0] + conv[1, :, 1, :] * tap[1][1]).T
    ready[1] = jnp.broadcast_to(as_col(tap[1][2]), (CH, B))
    ready[2] = jnp.broadcast_to(as_col(row_of(kept[2], 1)), (CH, B))
    for at, table in enumerate((bias, rate, skip)):
        ready[3, at : at + 1] = jnp.broadcast_to(of_head(row_of(table, 1)), (1, B))


def make_values(scaled, inv, far):
    outs = [pltpu.VMEM((4, CH, B), F32), pltpu.VMEM((B, N), F32)]
    outs += [pltpu.VMEM((B, 2, CH), F32), pltpu.VMEM((2, ROWS, D // 2), BF16), pltpu.VMEM((4, CH, B), F32)]
    outs += [pltpu.VMEM(*p) for p in KEPT]
    scratch = [pltpu.VMEM(*p) for p in (*NOW_FAR, *NEXT_FAR, ((ROWS, D), BF16))]
    scratch += [pltpu.SemaphoreType.DMA((8,)), pltpu.SemaphoreType.DMA((12,))]
    return call(values_kernel, "values", [scaled, inv], far, outs, scratch)


def advance(layer, push, direct, gate, writes, reads, state, w_out, gain, sent, states, scratch):
    fresh, decay_rows, read_rows, sems = scratch
    read_rows[...] = reads
    high, low = hi_lo(push)
    left = jnp.concatenate([high, high, low], axis=1)
    high, low = hi_lo(writes)
    right = jnp.concatenate([high, low, high], axis=0).astype(BF16)
    of = lax.broadcasted_iota(jnp.int32, left.shape, 1) % B
    left = jnp.concatenate([jnp.where(of == b, left, 0.0).astype(BF16) for b in range(B)], axis=0)
    pushed = jnp.dot(left, right, preferred_element_type=F32)
    lane = lax.broadcasted_iota(jnp.int32, (CH, B), 1)
    found = jnp.zeros((CH, B), F32)
    copies = []
    for b in range(B):
        new = decay_rows[b : b + 1, :] * state[b] + pushed[CH * b : CH * (b + 1)]
        fresh[b] = new
        total = jnp.sum(new * read_rows[b : b + 1, :], axis=1, keepdims=True)
        found = jnp.where(lane == b, total, found)
        if b % 8 == 7:
            part = pl.ds(b - 7, 8)
            copies.append(pltpu.make_async_copy(fresh.at[part], states.at[layer, part], sems.at[b // 8]))
            copies[-1].start()
    gated = (found + direct) * gate
    total = jnp.sum(gated * gated, axis=0, keepdims=True)
    high, low = hi_lo(total)
    tail = jnp.where(lax.broadcasted_iota(jnp.int32, (2, B), 0) == 0, high, low)
    tail = jnp.concatenate([tail, jnp.zeros((2, 128 - B), F32)], axis=1).astype(BF16)
    out = jnp.dot((gated * gain).T.astype(BF16), w_out[...], preferred_element_type=F32)
    for j in range(D // 128):
        to = LINES * (j ^ FIRST_MEMBER)
        sent[to : to + B] = out[:, 128 * j : 128 * j + 128].astype(BF16)
        sent[to + B : to + LINES] = tail
    for copy in copies:
        copy.wait()


STATES = ((2, B, CH, N), F32)
ADVANCE = (STATE, ((B, N), F32), ((B, N), F32))


def advance_scratch():
    return [pltpu.VMEM(*p) for p in ADVANCE] + [pltpu.SemaphoreType.DMA((4,))]


PLANE_SUMS = ((32 * LINES, 128), BF16)


def first_mix_kernel(keys, packed, decay, state, w_out, states, sent, weights, later, last_taps, lines, *scratch):
    for at in range(0, 4 * N, 16):
        pair = keys[at : at + 16].astype(F32)
        for half in range(2):
            to = (at + 8 * half) ^ (4 * FIRST_SPOT)
            lines[to : to + 8] = pair[8 * half : 8 * half + 8]
    weights[0] = lines[pl.ds(0, N, stride=4), :].astype(BF16)
    weights[1] = lines[pl.ds(1, N, stride=4), :].astype(BF16)
    first = lines[pl.ds(2, N, stride=4), :].T
    second = lines[pl.ds(3, N, stride=4), :].T
    later[0] = first[2 * B : 3 * B]
    later[1] = first[3 * B :]
    last_taps[...] = second[2 * B : 2 * B + 8]
    writes = first[:B] + second[:B]
    reads = first[B : 2 * B] + second[B : 2 * B]
    scratch[1][...] = decay[...]
    advance(
        0, packed[0], packed[1], packed[2], writes, reads, state, w_out, packed[3], sent, states, scratch
    )


def first_mix(keys, packed, decay, kept):
    return call(
        first_mix_kernel,
        "mix0",
        [keys, packed, decay, *kept],
        [],
        [
            pltpu.HBM(*STATES),
            pltpu.VMEM(*PLANE_SUMS),
            pltpu.VMEM((2, N, 128), BF16),
            pltpu.VMEM((2, B, N), F32),
            pltpu.VMEM((8, N), F32),
        ],
        [pltpu.VMEM((4 * N, 128), F32)] + advance_scratch(),
    )


def pack_kernel(own, packed):
    sums = [own[0, B * k : B * (k + 1)].astype(F32) for k in (1, 2)]
    packed[0] = own[0, :B]
    for at in range(1, 16):
        packed[at] = own[at, :B]
        for kind in range(2):
            sums[kind] += own[at, B * (kind + 1) : B * (kind + 2)].astype(F32)
    for kind in range(2):
        packed[16 + kind] = sums[kind].astype(BF16)


def take_half(half, side, norm_gain, weights, scaled, squares):
    for at in range(16):
        cols = pl.ds(pl.multiple_of(128 * (2 * (at ^ FIRST_CHIP) + side), 128), 128)
        part = half[at].astype(F32)
        squares += part * part
        scaled[:, 128 * at : 128 * at + 128] = (part * norm_gain[1:, cols]).astype(BF16)
    return squares, dot_nt(weights[side], scaled[...])


def half_kernel(own, weights, norm_gain, found_out, squares_out, sums_out, scaled):
    squares, found = take_half(own, lax.axis_index("c"), norm_gain, weights, scaled, jnp.zeros((B, N), F32))
    found_out[...] = found
    squares_out[...] = squares
    sums_out[0] = own[16].astype(F32)
    sums_out[1] = own[17].astype(F32)


HALF = ((B, D // 2), BF16)


def make_half(own, weights, norm_gain):
    outs = [pltpu.VMEM((ROWS, B), F32), pltpu.VMEM((B, N), F32), pltpu.VMEM((2, B, N), F32)]
    return call(half_kernel, "half", [own, weights, norm_gain], [], outs, [pltpu.VMEM(*HALF)])


def next_mix_kernel(other, weights, norm_gain, found, squares, sums, ready, later, last_taps, state, w_out, *refs):
    conv, key_conv, key_before, value_before = refs[:4]
    states, sent, key_out, value_out, scaled, *scratch = refs[5:]
    squares, rest = take_half(other, 1 - lax.axis_index("c"), norm_gain, weights, scaled, squares[...])
    sums = [sums[k] + other[16 + k].astype(F32) for k in range(2)]
    inv = lax.rsqrt(jnp.sum(squares, axis=1, keepdims=True) / D + EPS)
    found = (found[...] + rest) * as_row(inv)
    keys = [silu(later[k] + sums[k] * inv * (last_taps[2 * k : 2 * k + 1] + last_taps[2 * k + 1 : 2 * k + 2])) for k in range(2)]
    fresh_values = found[CH : 2 * CH]
    values = silu(ready[0] + fresh_values * ready[1])
    delta, decay = steps_of(found[2 * CH : 2 * CH + 1] + ready[3, :1], ready[3, 1:2])
    scratch[1][...] = jnp.broadcast_to(as_col(decay), (B, N))
    direct = ready[3, 2:3] * values
    advance(
        1, delta * values, direct, silu(found[:CH]), keys[0], keys[1], state, w_out, ready[2], sent, states, scratch
    )
    value_out[0] = value_before[...]
    value_out[1, :, 0, :] = conv[1, :, 1, :]
    value_out[1, :, 1, :] = fresh_values.T
    key_out[0] = key_before[...]
    for kind in range(2):
        key_out[1, 0, kind] = key_conv[1, 1, kind]
        key_out[1, 1, kind] = found[2 * CH + 8 + 4 * kind : 2 * CH + 12 + 4 * kind]


def next_mix(near, states):
    return call(
        next_mix_kernel,
        "mix1",
        near,
        [states],
        [
            pltpu.HBM(*STATES),
            pltpu.VMEM(*PLANE_SUMS),
            shaped((2, 2, 2, 4, B), F32),
            shaped((2, B, 2, CH), F32),
        ],
        [pltpu.VMEM(*HALF)] + advance_scratch(),
        {len(near): 0},
    )


def scale_kernel(got, sent):
    total = got[:B].astype(F32)
    squares = got[B:LINES].astype(F32)
    for j in range(1, 32):
        total += got[LINES * j : LINES * j + B].astype(F32)
        squares += got[LINES * j + B : LINES * (j + 1)].astype(F32)
    squares = squares[:1, :B] + squares[1:, :B]
    factor = as_col(lax.rsqrt(squares / GW + EPS))
    chunk = (total * factor).astype(BF16)
    for plane in range(8):
        sent[plane] = chunk


def make_scale(got):
    return call(scale_kernel, "scale", [got], [], [pltpu.VMEM((8, B, 128), BF16)])[0]


def first_add_kernel(got, hid, norm_gain, weights, sent):
    total = got[0].astype(F32)
    for plane in range(1, 8):
        total += got[plane].astype(F32)
    cols = pl.ds(pl.multiple_of(128 * lax.axis_index(PLANE), 128), 128)
    chunk = (hid[:, cols].astype(F32) + total).astype(BF16)
    scaled = (chunk.astype(F32) * norm_gain[1:, cols]).astype(BF16)
    shares = [dot_nt(scaled, weights[kind]).astype(BF16) for kind in range(2)]
    for j in range(16):
        sent[j, :B] = chunk
        sent[j, B : 2 * B] = shares[0]
        sent[j, 2 * B :] = shares[1]


def next_add_kernel(got, hid, sent):
    total = got[0].astype(F32)
    for plane in range(1, 8):
        total += got[plane].astype(F32)
    chunk = (hid[lax.axis_index(("y", "x")) ^ FIRST_CHIP].astype(F32) + total).astype(BF16)
    for j in range(32):
        sent[j] = chunk


def tokens_kernel(got, tokens_out):
    for j in range(32):
        at = 128 * (j ^ LAST_MEMBER)
        tokens_out[:, at : at + 128] = got[j]


def make_tokens(got):
    return call(tokens_kernel, "tokens", [got], [], [shaped((B, D), BF16)])[0]


def exchange(value, axes, first):
    order = [spot ^ first for spot in range(value.shape[0])]
    return lax.all_to_all(value, axes, 0, 0, axis_index_groups=[order], tiled=True)


def swap(value):
    return lax.ppermute(value, "c", [(0, 1), (1, 0)])


def per_device(
    tokens,
    norm_gain,
    w_gate,
    w_value,
    w_write,
    w_read,
    w_step,
    step_bias,
    decay_rate,
    skip_gain,
    conv_value_weight,
    conv_key_weight,
    group_gain,
    w_out,
    ssm_state,
    conv_value,
    conv_key,
):
    w_gate, w_value, w_write, w_read = (jnp.swapaxes(w, 1, 2) for w in (w_gate, w_value, w_write, w_read))
    conv_key = jnp.transpose(conv_key, (0, 2, 3, 4, 1))
    value_taps = jnp.swapaxes(conv_value_weight, 0, 1)
    far = [w_gate, w_value, w_step, w_write, w_read, ssm_state, w_out, group_gain, norm_gain]
    far += [step_bias, decay_rate, skip_gain, conv_value, value_taps, conv_key]
    key_far = [w_write, w_read, conv_key, conv_key_weight]
    others = [swap(v) for v in key_far]
    scaled, inv, hid, *own = make_start(tokens, norm_gain, key_far)
    msg, key_out = make_keys(scaled, inv, own, others)
    keys = exchange(msg, ("z", "y", "x"), FIRST_SPOT).reshape(4 * N, 128)
    packed, decay, value_out, halves, ready, *kept = make_values(scaled, inv, far)
    state, out, gain, next_state, next_out, *rest = kept
    states, sent, weights, later, last_taps = first_mix(keys, packed, decay, [state, out])
    sent = make_scale(exchange(sent.reshape(32, LINES // 2, 2, 128), PLANE, FIRST_MEMBER).reshape(sent.shape))
    (sent,) = call(
        first_add_kernel,
        "add0",
        [exchange(sent, ("z",), FIRST_PLANE), hid, rest[0], weights],
        [],
        [pltpu.VMEM((16, 3 * B, 128), BF16)],
    )
    own = exchange(sent, ("y", "x"), FIRST_CHIP)
    (own,) = call(pack_kernel, "pack", [own], [], [pltpu.VMEM((18, B, 128), BF16)])
    other = swap(own)
    norm_far, conv, key_conv = rest[0], rest[4], rest[6]
    half = make_half(own, halves, norm_far)
    near = [other, halves, norm_far, *half, ready, later, last_taps, next_state, next_out]
    states, sent, key_out, value_out = next_mix([*near, conv, key_conv, key_out, value_out], states)
    sent = make_scale(exchange(sent.reshape(32, LINES // 2, 2, 128), PLANE, FIRST_MEMBER).reshape(sent.shape))
    (sent,) = call(next_add_kernel, "add1", [exchange(sent, ("z",), FIRST_PLANE), own], [], [pltpu.VMEM((32, B, 128), BF16)])
    hid = exchange(sent, PLANE, LAST_MEMBER)
    tokens_out = make_tokens(hid)
    return (tokens_out, states, value_out, jnp.transpose(key_out, (0, 4, 1, 2, 3)))


def solution(mesh):
    torus = Mesh(mesh.devices.reshape(8, 4, 4, 2), TP)
    in_specs = (
        P(),
        P(),
        P(None, None, TP),
        P(None, None, TP),
        P(None, None, TP),
        P(None, None, TP),
        P(),
        P(),
        P(),
        P(),
        P(None, None, TP),
        P(None, None, None, TP),
        P(None, TP),
        P(None, TP, None),
        P(None, None, TP, None),
        P(None, None, None, TP),
        P(None, None, None, None, TP),
    )
    out_specs = (
        P(),
        P(None, None, TP, None),
        P(None, None, None, TP),
        P(None, None, None, None, TP),
    )
    return jax.shard_map(
        per_device, mesh=torus, in_specs=in_specs, out_specs=out_specs, check_vma=False
    )
```
